256 devices in a mesh: ep: 64 (over z, y, core), tp: 4 (over x).
Axes of the slice: x: 4, y: 4, z: 8, core: 2. Of those that a mesh axis runs over, the one named last changes fastest.
Arguments:
- queries: bfloat16 [8192, 512], P('ep', 'tp'), may hold values from -8 to 8
- key_cache: bfloat16 [4, 64, 8192], P('tp', None, 'ep'), may hold values from -4.5 to 4.5
- value_cache: bfloat16 [4, 64, 8192], P('tp', None, 'ep'), may hold values from -6 to 6
- cum_gate: float32 [4, 8192], P('tp'), may hold values from -2048 to 0, as said below
- out_weight: bfloat16 [512, 2048], replicated, may hold values from -1 to 1
- routed_input: bfloat16 [16384, 2048], P('ep'), may hold values from -6 to 6
- norm_gain: bfloat16 [2048], replicated, may hold values from 0.099609375 to 1.8984375
- routes: int32 [16384, 2], P('ep'), may hold values from 0 to 63, all different within a row; in each aligned block of 64 rows (0 to 63, 64 to 127, ...) at most 3 rows name the same one
- route_weight: float32 [16384, 2], P('ep'), may hold values from 0.2 to 1
- expert_gate: bfloat16 [64, 2048, 1024], P('ep', None, 'tp'), may hold values from -0.125 to 0.125
- expert_up: bfloat16 [64, 2048, 1024], P('ep', None, 'tp'), may hold values from -0.125 to 0.125
- expert_down: bfloat16 [64, 1024, 2048], P('ep', 'tp'), may hold values from -0.1875 to 0.1875
Outputs:
- mixed_out: bfloat16 [8192, 2048], P(('ep', 'tp'))
- expert_out: bfloat16 [16384, 2048], P(('ep', 'tp'))
The draws below stay inside these ranges and needn't reach their ends.
Inputs may be any that keep to these rules, and one draw needn't show every extreme that they name: `cum_gate`: Non-increasing along positions in every head. `routes`: each row names 2 different experts. In each aligned block of 64 rows (the rows of one device) no expert is named by more than 3 rows, a bound that some block reaches.
All inputs are finite; a program needn't handle non-finite values.
Results may differ from the reference program's by a relative error of at most 0.012.
Values may be sent and summed in bfloat16 or wider, within the bound.
A program may use at most 64 MiB of HBM per device.

```python
import math
import jax
import jax.numpy as jnp
import numpy as np
from jax import lax

D = 2048
HEADS = 8
HEAD = 64
KV_HEADS = 4
FFE = 1024
TOPK = 2
SEQ_ROWS = 128
TOK_DEV = 64
FIRST_TOKENS = 8192
ROUTED_TOKENS = 16384
EXPERTS = 64
CAP = 3
N_TP = 4


def draw_queries(key, part):
    base_key = jax.random.fold_in(key, 11)
    values = jnp.clip(jax.random.normal(base_key, (FIRST_TOKENS, HEADS * HEAD), jnp.float32), -4.0, 4.0)
    return values.astype(jnp.bfloat16)


def draw_key_cache(key, part):
    base_key = jax.random.fold_in(key, 13)
    values = jnp.clip(jax.random.normal(base_key, (KV_HEADS, HEAD, FIRST_TOKENS), jnp.float32), -4.0, 4.0)
    return values.astype(jnp.bfloat16)


def draw_cum_gate(key, part):
    ordering_random_key, gradual_random_key, quick_random_key, block_random_key, coarse_random_key, spike_random_key, loss_random_key = jax.random.split(jax.random.fold_in(key, 17), 7)
    ranks = jax.random.permutation(ordering_random_key, KV_HEADS)
    gradual_decay = ranks < KV_HEADS // 2
    rough = jax.random.uniform(coarse_random_key, (KV_HEADS, FIRST_TOKENS), jnp.float32, 0.2, 1.8)
    slow_rate = jax.random.uniform(gradual_random_key, (KV_HEADS,), jnp.float32, 0.1, 0.4) / FIRST_TOKENS
    fast_rate = 1.0 / jax.random.uniform(quick_random_key, (KV_HEADS,), jnp.float32, 30.0, 100.0)
    rate = jnp.where(gradual_decay, slow_rate, fast_rate)
    factor = jnp.exp(jax.random.uniform(block_random_key, (FIRST_TOKENS // SEQ_ROWS,), jnp.float32, -0.7, 0.7))
    per_position = jnp.repeat(factor, SEQ_ROWS)
    update_steps = -rate[:, None] * per_position[None, :] * rough
    marked_positions = jax.random.randint(spike_random_key, (2,), 0, FIRST_TOKENS)
    loss_values = jnp.log(jax.random.uniform(loss_random_key, (2,), jnp.float32, 0.5, 0.8))
    sudden_spike = jnp.zeros((FIRST_TOKENS,), jnp.float32).at[marked_positions].add(loss_values)
    update_steps = update_steps + jnp.where(gradual_decay[:, None], sudden_spike[None, :], 0.0)
    return jnp.cumsum(update_steps, axis=1)


def block_scale(stream_key, shape, cuts, low, largest):
    gain, own = 1.0, jax.random.fold_in(stream_key, 6)
    for dim, shards_of in cuts:
        draws = jnp.exp(jax.random.uniform(jax.random.fold_in(own, dim), (shards_of,), jnp.float32, low / len(cuts), largest / len(cuts)))
        gain = gain * jnp.repeat(draws, shape[dim] // shards_of).reshape([-1 if axis == dim else 1 for axis in range(len(shape))])
    return gain


def routed_block(stream_key, own, number, rows, count, top, bound, lean):
    order = jax.random.permutation(stream_key, count)
    packed, usual = load_shares(count, rows * top, bound, lean, True), load_shares(count, rows * top, bound, lean, False)
    places = jnp.arange(count)

    def named(sizes, turn):
        used = int((sizes > 0).sum())
        fixed = max(1, used // 4)
        passed = fixed + (places - fixed + turn * (used - fixed)) % max(1, count - fixed)
        return jnp.zeros((count,), jnp.int32).at[order[jnp.where(places < fixed, places, passed)]].set(jnp.asarray(sizes, jnp.int32))

    sizes = jnp.where(number % 4 == 0, named(packed, number // 4), named(usual, number - number // 4 - 1))
    mixed = jax.random.permutation(jax.random.fold_in(own, 3), count)
    donor, taker = mixed[0:count // 2 * 2:2], mixed[1:count // 2 * 2:2]
    margin = jnp.minimum(sizes[donor] - 1, bound - sizes[taker]) // 2
    margin = jnp.where((donor == order[0]) | (taker == order[0]) | (sizes[taker] == 0), 0, jnp.maximum(margin, 0))
    passed = jax.random.randint(jax.random.fold_in(own, 4), (count // 2,), 0, 1 << 20) % (margin + 1)
    sizes = sizes.at[donor].add(-passed).at[taker].add(passed)
    members = jnp.searchsorted(jnp.cumsum(sizes), jnp.arange(rows * top), side="right").astype(jnp.int32)
    table = members.reshape(top, rows).T
    table = table[jax.random.permutation(jax.random.fold_in(own, 1), rows)]
    turn = jax.random.randint(jax.random.fold_in(own, 2), (rows, 1), 0, top)
    return jnp.take_along_axis(table, (jnp.arange(top)[None, :] + turn) % top, axis=1)


def load_shares(amount, total, bound, slope, full):
    loads = [(1 << 20) // math.isqrt(rank ** slope) + 1 for rank in range(1, amount + 1)]
    largest = bound if full else min(bound, max(-(-total // amount), total * loads[0] // sum(loads)))
    least = 1 if total - largest >= amount - 1 else 0
    counts, spare = [largest] + [least] * (amount - 1), total - largest - least * (amount - 1)
    while spare > 0:
        movable = [i for i in range(1, amount) if counts[i] < largest] or [i for i in range(1, amount) if counts[i] < bound]
        whole, budget = sum([loads[i] for i in movable]), spare
        for i in movable:
            addition = min(bound - counts[i], max(1, budget * loads[i] // whole), spare)
            counts[i] = counts[i] + addition
            spare = spare - addition
    return np.array(counts)


def centred(key, dims, spread, bound, pieces=(), kind=jnp.bfloat16):
    result = jax.random.normal(key, dims, jnp.float32) * spread
    if len(pieces) > 0:
        result = block_scale(key, dims, pieces, -0.22, 0.18) * result
    return jnp.clip(result, min=-bound, max=bound).astype(kind)


def setup_inputs(seed: int = 0) -> dict:
    keys = jax.random.split(jax.random.key(seed), 13)
    queries = draw_queries(jax.random.fold_in(keys[12], 71), 0)
    key_cache = draw_key_cache(jax.random.fold_in(keys[12], 71), 0)
    value_cache = centred(keys[2], (KV_HEADS, HEAD, FIRST_TOKENS), 1.0, 6.0, ((0, 4), (2, 64)))
    cum_gate = draw_cum_gate(jax.random.fold_in(keys[12], 71), 0)
    out_weight = centred(keys[4], (HEADS * HEAD, D), (HEADS * HEAD // 16) ** -0.5, 1.0)
    routed_input = centred(keys[5], (ROUTED_TOKENS, D), 1.0, 6.0, ((0, 64),))
    norm_gain = jnp.clip(1.0 + 0.18 * jax.random.normal(keys[6], (D,), jnp.float32), 0.099609375, 1.8984375).astype(jnp.bfloat16)
    routes_keys = jax.random.split(jax.random.fold_in(keys[7], 1), ROUTED_TOKENS // TOK_DEV)
    routes_turns = jax.random.permutation(jax.random.fold_in(keys[7], 3), ROUTED_TOKENS // TOK_DEV)
    routes = jax.vmap(lambda own, number: routed_block(jax.random.fold_in(keys[7], 2), own, number, TOK_DEV, EXPERTS, TOPK, CAP, 1))(routes_keys, routes_turns).reshape((ROUTED_TOKENS, TOPK))
    route_weight = jnp.clip(0.2 + 0.8 * jax.random.uniform(keys[8], (ROUTED_TOKENS, TOPK), jnp.float32) ** block_scale(keys[8], (ROUTED_TOKENS, TOPK), ((0, 64),), -0.2, 0.2), 0.2, 1.0)
    expert_gate = centred(keys[9], (EXPERTS, D, FFE), D ** -0.5, 0.125, ((0, 64), (2, 4)))
    expert_up = centred(keys[10], (EXPERTS, D, FFE), D ** -0.5, 0.125, ((0, 64), (2, 4)))
    expert_down = centred(keys[11], (EXPERTS, FFE, D), FFE ** -0.5, 0.1875, ((0, 64), (1, 4)))
    return dict(queries=queries, key_cache=key_cache, value_cache=value_cache, cum_gate=cum_gate, out_weight=out_weight, routed_input=routed_input, norm_gain=norm_gain, routes=routes, route_weight=route_weight, expert_gate=expert_gate, expert_up=expert_up, expert_down=expert_down)


def attend_block(query_block, keys_head, values_head, gate_head, block_start):
    rows_here = query_block.shape[0]
    scores = jnp.einsum('tgd,ds->tgs', query_block, keys_head) * HEAD ** (-0.5)
    query_pos = block_start + jnp.arange(rows_here, dtype=jnp.int32)
    gate_query = lax.dynamic_slice_in_dim(gate_head, block_start, rows_here, 0)
    scores = scores + gate_query[:, None, None] - gate_head[None, None, :]
    key_pos = jnp.arange(FIRST_TOKENS, dtype=jnp.int32)
    allowed = key_pos[None, :] <= query_pos[:, None]
    scores = jnp.where(allowed[:, None, :], scores, -jnp.inf)
    highest = lax.optimization_barrier(jnp.max(scores, axis=-1, keepdims=True))
    weights = jnp.exp(scores - highest)
    total = lax.optimization_barrier(jnp.sum(weights, axis=-1))
    rounded = lax.optimization_barrier(weights.astype(jnp.bfloat16)).astype(jnp.float32)
    summed = jnp.einsum('tgs,ds->tgd', rounded, values_head)
    return (summed / total[..., None]).astype(jnp.bfloat16)

def reference(queries, key_cache, value_cache, cum_gate, out_weight, routed_input, norm_gain, routes, route_weight, expert_gate, expert_up, expert_down):
    group = HEADS // KV_HEADS
    nblocks = FIRST_TOKENS // SEQ_ROWS
    query_all = queries.astype(jnp.float32).reshape(nblocks, SEQ_ROWS, KV_HEADS, group, HEAD)
    keys_all = key_cache.astype(jnp.float32)
    values_all = value_cache.astype(jnp.float32)

    def one_pair(index):
        block = index // KV_HEADS
        head = index % KV_HEADS
        query_block = query_all[block, :, head]
        start = (block * SEQ_ROWS).astype(jnp.int32)
        return attend_block(query_block, keys_all[head], values_all[head], cum_gate[head], start)
    attended = lax.map(one_pair, jnp.arange(nblocks * KV_HEADS, dtype=jnp.int32))
    attended = attended.reshape(nblocks, KV_HEADS, SEQ_ROWS, group, HEAD).transpose(0, 2, 1, 3, 4).reshape(FIRST_TOKENS, HEADS * HEAD)
    mixed_out = jnp.dot(attended, out_weight, preferred_element_type=jnp.float32).astype(jnp.bfloat16)
    source = routed_input.astype(jnp.float32)
    scale = lax.rsqrt(lax.optimization_barrier(jnp.mean(source * source, axis=-1, keepdims=True)) + 1e-06)
    normed = (source * scale * norm_gain.astype(jnp.float32)).astype(jnp.bfloat16)
    nparts = ROUTED_TOKENS // TOK_DEV
    slots_all = EXPERTS * CAP
    pairs = routes.reshape(nparts, TOK_DEV * TOPK)
    same = (pairs[:, :, None] == jnp.arange(EXPERTS, dtype=jnp.int32)[None, None, :]).astype(jnp.int32)
    earlier = jnp.cumsum(same, axis=1) - same
    rank = lax.optimization_barrier(jnp.sum(earlier * same, axis=2))
    slot = pairs * CAP + rank
    chooser = (slot[:, :, None] == jnp.arange(slots_all, dtype=jnp.int32)[None, None, :]).astype(jnp.float32)
    chooser = chooser.reshape(nparts, TOK_DEV, TOPK, slots_all)
    normed_blocks = normed.astype(jnp.float32).reshape(nparts, TOK_DEV, D)
    width_part = FFE // N_TP

    def one_expert(expert):
        picks = lax.dynamic_slice_in_dim(chooser, expert * CAP, CAP, 3)
        gathered = jnp.einsum('btkc,btd->bcd', picks, normed_blocks).astype(jnp.bfloat16).reshape(nparts * CAP, D)
        gate = jnp.dot(gathered, expert_gate[expert], preferred_element_type=jnp.float32)
        upper = jnp.dot(gathered, expert_up[expert], preferred_element_type=jnp.float32)
        hidden = (jax.nn.silu(gate) * upper).astype(jnp.bfloat16)
        hidden_parts = hidden.astype(jnp.float32).reshape(nparts * CAP, N_TP, width_part)
        down_parts = expert_down[expert].astype(jnp.float32).reshape(N_TP, width_part, D)
        partial_value = jnp.einsum('rqf,qfd->qrd', hidden_parts, down_parts)
        partial_value = lax.optimization_barrier(partial_value.astype(jnp.bfloat16)).astype(jnp.float32)
        return lax.optimization_barrier(jnp.sum(partial_value, axis=0)).astype(jnp.bfloat16).reshape(nparts, CAP, D)
    results = lax.map(one_expert, jnp.arange(EXPERTS, dtype=jnp.int32))
    rank_blocks = rank.reshape(nparts, TOK_DEV, TOPK)
    expert_blocks = routes.reshape(nparts, TOK_DEV, TOPK)
    block_ids = jnp.arange(nparts, dtype=jnp.int32)[:, None, None]
    picked = results[expert_blocks, block_ids, rank_blocks].astype(jnp.float32)
    mixed_weights = route_weight.reshape(nparts, TOK_DEV, TOPK)[..., None] * picked
    expert_out = lax.optimization_barrier(jnp.sum(mixed_weights, axis=2)).reshape(ROUTED_TOKENS, D).astype(jnp.bfloat16)
    return (mixed_out, expert_out)
```

```python
import functools

import jax
import jax.numpy as jnp
from jax import lax
from jax.experimental import pallas as pl
from jax.experimental.pallas import tpu as pltpu
from jax.sharding import PartitionSpec as P

MESH = pl.DeviceIdType.MESH
BF = jnp.bfloat16
F32 = jnp.float32

D = 2048
ROWS = 64
CAP = 3
NT = 4
NZ = 8
NYC = 8
NE = NZ * NYC
SL = NE * CAP
TR = D // 128
CH = CAP * TR
QR = NYC * CH
ALL = NE * CH
NP = NZ // 2
PT = 2 * NYC * CAP
HID = 256
DZ = (0, 1, 7, 2, 6, 3, 5, 4)


def permutation():
    a = lax.broadcasted_iota(jnp.int32, (256, 256), 0)
    b = lax.broadcasted_iota(jnp.int32, (256, 256), 1)
    hit = ((a & 15) == (b >> 4)) & ((a >> 4) == (b & 15))
    return hit.astype(F32).astype(BF)


def mm(a, b):
    return jnp.dot(a, b, preferred_element_type=F32)


def rows_to_tiles(perm, src, row, dst, at):
    z = jnp.concatenate([src[row : row + 16, 128 * i : 128 * i + 128] for i in range(TR)], axis=0)
    dst[at : at + 256, :] = mm(perm, z).astype(BF)


def moe_kernel(
    x_hbm, routes_ref, rw_ref, gain_ref, wg_hbm, wu_hbm, wd_hbm,
    out_ref,
    xin, obuf, pick, send, recv, wg, wu, wd, xb, part, rs1, rss, rsd, sumb, tot, ret, back, resb,
    ld_sem, as_sem, a_sem, xs_sem, gl_sem, gr_sem, g2_sem, rr_sem, r1_sem, rss_sem, rsd_sem, bs_sem, b_sem,
):
    t = lax.axis_index("tp")
    me = lax.axis_index("ep")
    z = me // NYC
    yc = me % NYC
    right = (t + 1) % NT
    left = (t + 3) % NT
    opp = (t + 2) % NT

    loads = [
        pltpu.make_async_copy(x_hbm.at[pl.ds(pl.multiple_of(t * ROWS, ROWS), ROWS), :], xin, ld_sem.at[0]),
        pltpu.make_async_copy(wg_hbm, wg, ld_sem.at[1]),
        pltpu.make_async_copy(wu_hbm, wu, ld_sem.at[2]),
        pltpu.make_async_copy(wd_hbm, wd, ld_sem.at[3]),
    ]
    for c in loads:
        c.start()

    barrier = pltpu.get_barrier_semaphore()

    def greet(k, _):
        pl.semaphore_signal(barrier, inc=1, device_id=((me + k) % NE, t), device_id_type=MESH)
        return 0

    lax.fori_loop(1, NE, greet, 0)
    for x in (right, left):
        pl.semaphore_signal(barrier, inc=1, device_id=(me, x), device_id_type=MESH)

    perm = permutation()

    own = pl.ds(pl.multiple_of(t * ROWS, ROWS), ROWS)
    r = routes_ref[own, :]
    r0 = r[:, 0:1]
    r1 = r[:, 1:2]
    lane = lax.broadcasted_iota(jnp.int32, (ROWS, NE), 1)
    s0 = jnp.where(r0 == lane, 1.0, 0.0)
    s1 = jnp.where(r1 == lane, 1.0, 0.0)
    low = jnp.where(
        lax.broadcasted_iota(jnp.int32, (ROWS, ROWS), 0) > lax.broadcasted_iota(jnp.int32, (ROWS, ROWS), 1), 1.0, 0.0
    )
    before = mm(low.astype(BF), (s0 + s1).astype(BF))
    k0 = jnp.sum(before * s0, axis=1, keepdims=True)
    k1 = jnp.sum((before + s0) * s1, axis=1, keepdims=True)
    slots = lax.broadcasted_iota(jnp.int32, (ROWS, SL), 1).astype(F32)
    c0 = jnp.where(r0.astype(F32) * CAP + k0 == slots, 1.0, 0.0)
    c1 = jnp.where(r1.astype(F32) * CAP + k1 == slots, 1.0, 0.0)
    pick[0:ROWS, :] = c0.astype(BF)
    pick[ROWS : 2 * ROWS, :] = c1.astype(BF)

    loads[0].wait()
    wide = xin[...].astype(F32)
    scale = lax.rsqrt(jnp.mean(wide * wide, axis=-1, keepdims=True) + 1e-06)
    normed = (wide * scale * gain_ref[...].astype(F32)).astype(BF)
    chosen = jnp.transpose(c0 + c1).astype(BF)
    obuf[...] = mm(chosen, normed).astype(BF)
    for g in range(SL // 16):
        rows_to_tiles(perm, obuf, 16 * g, send, 256 * g)

    pl.semaphore_wait(barrier, NE - 1 + 2)

    for q in range(NZ):
        far = ((z + DZ[q]) % NZ) * NYC

        def ship(j, _, q=q, far=far):
            to = far + (yc + j) % NYC
            pltpu.make_async_remote_copy(
                src_ref=send.at[pl.ds(pl.multiple_of(to * CH, CH), CH), :],
                dst_ref=recv.at[t, pl.ds(pl.multiple_of(q * QR + yc * CH, CH), CH), :],
                send_sem=as_sem,
                recv_sem=a_sem.at[q],
                device_id=(to, t),
                device_id_type=MESH,
            ).start()
            return 0

        lax.fori_loop(1 if q == 0 else 0, NYC, ship, 0)
    recv[t, pl.ds(pl.multiple_of(yc * CH, CH), CH), :] = send[pl.ds(pl.multiple_of(me * CH, CH), CH), :]

    def chunk(src, q):
        return recv.at[src, pl.ds(q * QR, QR), :]

    def hop(src, q, sem, x):
        return pltpu.make_async_remote_copy(
            src_ref=chunk(src, q), dst_ref=chunk(src, q), send_sem=xs_sem, recv_sem=sem.at[q],
            device_id=(me, x), device_id_type=MESH,
        )

    def arrive(q):
        n = QR - CH if q == 0 else QR
        pltpu.make_async_remote_copy(
            src_ref=send.at[pl.ds(0, n), :], dst_ref=recv.at[t, pl.ds(q * QR, n), :],
            send_sem=as_sem, recv_sem=a_sem.at[q], device_id=(me, right), device_id_type=MESH,
        ).wait_recv()

    def spread(q):
        arrive(q)
        hop(t, q, gl_sem, right).start()
        hop(t, q, gr_sem, left).start()

    def relay(q):
        if q % 2 == 0:
            hop(left, q, gl_sem, right).wait_recv()
            hop(left, q, g2_sem, right).start()
        else:
            hop(right, q, gr_sem, left).wait_recv()
            hop(right, q, g2_sem, left).start()

    def gathered(q):
        if q % 2 == 0:
            hop(right, q, gr_sem, left).wait_recv()
        else:
            hop(left, q, gl_sem, right).wait_recv()
        hop(opp, q, g2_sem, right).wait_recv()

    def rsend(src, dst, sem, p, x):
        return pltpu.make_async_remote_copy(
            src_ref=src, dst_ref=dst.at[p], send_sem=rr_sem, recv_sem=sem.at[p], device_id=(me, x), device_id_type=MESH
        )

    def ways(p):
        return (right, left) if p % 2 == 0 else (left, right)

    def experts(p):
        gathered(2 * p)
        gathered(2 * p + 1)
        if p == 0:
            for c in loads[1:]:
                c.wait()
        for tt in range(NT):
            for g in range(PT // 16):
                at = p * 2 * QR + g * 256
                y = mm(perm, recv[tt, at : at + 256, :]).astype(BF)
                row = tt * PT + 16 * g
                for i in range(TR):
                    xb[row : row + 16, 128 * i : 128 * i + 128] = y[16 * i : 16 * i + 16, :]
        x = xb[...]
        gate = mm(x, wg[...])
        up = mm(x, wu[...])
        hidden = (gate / (1.0 + jnp.exp(-gate)) * up).astype(BF)
        for tt in range(NT):
            part[p, tt] = mm(hidden[tt * PT : (tt + 1) * PT, :], wd[...]).astype(BF)
        fwd, bwd = ways(p)
        rsend(part.at[p, opp], rs1, r1_sem, p, fwd).start()
        rsend(part.at[p, bwd], rss, rss_sem, p, bwd).start()

    def middle(p):
        fwd, bwd = ways(p)
        rsend(part.at[p, opp], rs1, r1_sem, p, fwd).wait_recv()
        sumb[p] = (rs1[p].astype(F32) + part[p, fwd].astype(F32)).astype(BF)
        rsend(sumb.at[p], rsd, rsd_sem, p, fwd).start()

    def finish(p):
        fwd, bwd = ways(p)
        rsend(part.at[p, bwd], rss, rss_sem, p, bwd).wait_recv()
        rsend(sumb.at[p], rsd, rsd_sem, p, fwd).wait_recv()
        tot[...] = (part[p, t].astype(F32) + rss[p].astype(F32) + rsd[p].astype(F32)).astype(BF)
        for g in range(PT // 16):
            rows_to_tiles(perm, tot, 16 * g, ret, p * 2 * QR + 256 * g)
        for q in (2 * p, 2 * p + 1):
            far = ((z + NZ - DZ[q]) % NZ) * NYC

            def home(j, _, q=q, far=far):
                to = (yc + j) % NYC
                pltpu.make_async_remote_copy(
                    src_ref=ret.at[pl.ds(pl.multiple_of(q * QR + to * CH, CH), CH), :],
                    dst_ref=back.at[pl.ds(pl.multiple_of(me * CH, CH), CH), :],
                    send_sem=bs_sem,
                    recv_sem=b_sem,
                    device_id=(far + to, t),
                    device_id_type=MESH,
                ).start()
                return 0

            lax.fori_loop(1 if q == 0 else 0, NYC, home, 0)
        if p == 0:
            back[pl.ds(pl.multiple_of(me * CH, CH), CH), :] = ret[pl.ds(pl.multiple_of(yc * CH, CH), CH), :]

    for step in (
        (spread, 0), (spread, 1), (relay, 0), (spread, 2), (relay, 1), (spread, 3), (relay, 2), (experts, 0),
        (spread, 4), (relay, 3), (spread, 5), (relay, 4), (experts, 1), (spread, 6), (relay, 5), (spread, 7),
        (relay, 6), (relay, 7), (middle, 0), (experts, 2), (middle, 1), (finish, 0), (experts, 3), (middle, 2),
        (finish, 1), (middle, 3), (finish, 2), (finish, 3),
    ):
        step[0](step[1])

    n = ALL - CH
    last = pltpu.make_async_remote_copy(
        src_ref=ret.at[pl.ds(0, n), :], dst_ref=back.at[pl.ds(0, n), :], send_sem=bs_sem, recv_sem=b_sem,
        device_id=(me, right), device_id_type=MESH,
    )
    last.wait_recv()
    for g in range(SL // 16):
        y = mm(perm, back[256 * g : 256 * g + 256, :]).astype(BF)
        for i in range(TR):
            resb[16 * g : 16 * g + 16, 128 * i : 128 * i + 128] = y[16 * i : 16 * i + 16, :]
    picked = mm(pick[...], resb[...])
    w = rw_ref[own, :]
    out_ref[...] = (w[:, 0:1] * picked[0:ROWS, :] + w[:, 1:2] * picked[ROWS : 2 * ROWS, :]).astype(BF)

    last.wait_send()
    pltpu.make_async_remote_copy(
        src_ref=send.at[pl.ds(0, n), :], dst_ref=recv.at[t, pl.ds(0, n), :], send_sem=as_sem, recv_sem=a_sem.at[0],
        device_id=(me, right), device_id_type=MESH,
    ).wait_send()
    pltpu.make_async_remote_copy(
        src_ref=recv.at[pl.ds(0, 3)], dst_ref=recv.at[pl.ds(0, 3)], send_sem=xs_sem, recv_sem=gl_sem.at[0],
        device_id=(me, right), device_id_type=MESH,
    ).wait_send()
    pltpu.make_async_remote_copy(
        src_ref=part.at[:, pl.ds(0, 3)], dst_ref=part.at[:, pl.ds(0, 3)], send_sem=rr_sem, recv_sem=r1_sem.at[0],
        device_id=(me, right), device_id_type=MESH,
    ).wait_send()


def expert_half(routed_input, norm_gain, routes, route_weight, expert_gate, expert_up, expert_down):
    vmem = pl.BlockSpec(memory_space=pltpu.VMEM)
    hbm = pl.BlockSpec(memory_space=pl.ANY)
    dma = pltpu.SemaphoreType.DMA
    return pl.pallas_call(
        moe_kernel,
        out_shape=jax.ShapeDtypeStruct((ROWS, D), BF),
        in_specs=[hbm, vmem, vmem, vmem, hbm, hbm, hbm],
        out_specs=vmem,
        scratch_shapes=[
            pltpu.VMEM((ROWS, D), BF),
            pltpu.VMEM((SL, D), BF),
            pltpu.VMEM((2 * ROWS, SL), BF),
            pltpu.VMEM((ALL, 128), BF),
            pltpu.VMEM((NT, ALL, 128), BF),
            pltpu.VMEM((D, HID), BF),
            pltpu.VMEM((D, HID), BF),
            pltpu.VMEM((HID, D), BF),
            pltpu.VMEM((NT * PT, D), BF),
            pltpu.VMEM((NP, NT, PT, D), BF),
            pltpu.VMEM((NP, PT, D), BF),
            pltpu.VMEM((NP, PT, D), BF),
            pltpu.VMEM((NP, PT, D), BF),
            pltpu.VMEM((NP, PT, D), BF),
            pltpu.VMEM((PT, D), BF),
            pltpu.VMEM((ALL, 128), BF),
            pltpu.VMEM((ALL, 128), BF),
            pltpu.VMEM((SL, D), BF),
            dma((4,)),
            dma,
            dma((NZ,)),
            dma,
            dma((NZ,)),
            dma((NZ,)),
            dma((NZ,)),
            dma,
            dma((NP,)),
            dma((NP,)),
            dma((NP,)),
            dma,
            dma,
        ],
        compiler_params=pltpu.CompilerParams(
            collective_id=0, has_side_effects=True, vmem_limit_bytes=40 * 1024 * 1024
        ),
        cost_estimate=pl.CostEstimate(flops=60_000_000_000, bytes_accessed=8_000_000, transcendentals=0),
        name="experts",
    )(
        routed_input, routes, route_weight, norm_gain.reshape(1, D),
        expert_gate[0], expert_up[0], expert_down[0],
    )
def side_by_side(arrays, axis, dim, along):
    both = jnp.concatenate(arrays, axis=along)
    out, at, gathered = (lax.all_gather(both, axis, axis=dim, tiled=True), 0, [])
    for a in arrays:
        gathered.append(lax.slice_in_dim(out, at, at + a.shape[along], axis=along))
        at += a.shape[along]
    return tuple(gathered)


def mixer_half(queries, key_cache, value_cache, cum_gate, out_weight):
    seq_rows = queries.shape[0]
    local_heads = key_cache.shape[0]
    head_size = key_cache.shape[1]
    group = queries.shape[1] // (local_heads * head_size)
    own_start = lax.axis_index("ep") * seq_rows
    query_heads = queries.reshape(seq_rows, local_heads, group, head_size)
    query_pos = own_start + jnp.arange(seq_rows, dtype=jnp.int32)
    gate_query = lax.dynamic_slice_in_dim(cum_gate, own_start, seq_rows, 1)
    gate_rows = jnp.transpose(gate_query)[:, :, None, None]
    scale = head_size ** (-0.5)
    best_start = jnp.full((seq_rows, local_heads, group), -jnp.inf, jnp.float32)
    total_start = jnp.zeros((seq_rows, local_heads, group), jnp.float32)
    summed_start = jnp.zeros((seq_rows, local_heads * group * head_size), jnp.float32)
    pieces = side_by_side((key_cache, value_cache), "ep", 2, 0)

    def update(state):
        best, total, summed = state
        key_piece, value_piece = pieces
        width = key_piece.shape[2]
        scores = (
            jnp.einsum("thgd,hds->thgs", query_heads, key_piece, preferred_element_type=jnp.float32)
            * scale
        )
        scores = scores + gate_rows - cum_gate[None, :, None, :]
        key_pos = jnp.arange(width, dtype=jnp.int32)
        allowed = key_pos[None, :] <= query_pos[:, None]
        scores = jnp.where(allowed[:, None, None, :], scores, -jnp.inf)
        new_best = jnp.max(scores, axis=-1)
        factor = jnp.exp(best - new_best)
        weights = jnp.exp(scores - new_best[..., None])
        new_total = total * factor + jnp.sum(weights, axis=-1)
        product = jnp.einsum(
            "thgs,hds->thgd",
            weights.astype(jnp.bfloat16),
            value_piece,
            preferred_element_type=jnp.float32,
        )
        new_summed = summed.reshape(product.shape) * factor[..., None] + product
        return (new_best, new_total, new_summed.reshape(seq_rows, local_heads * group * head_size))

    best, total, summed = lax.cond(
        jnp.int32(0) <= own_start,
        update,
        lambda state: state,
        (best_start, total_start, summed_start),
    )
    attended = summed.reshape(seq_rows, local_heads, group, head_size) / total[..., None]
    attended = attended.astype(jnp.bfloat16).reshape(seq_rows, local_heads * group * head_size)
    by_position = lax.all_to_all(attended, "tp", split_axis=0, concat_axis=1, tiled=True)
    return jnp.dot(by_position, out_weight, preferred_element_type=jnp.float32).astype(jnp.bfloat16)


def body(
    queries,
    key_cache,
    value_cache,
    cum_gate,
    out_weight,
    routed_input,
    norm_gain,
    routes,
    route_weight,
    expert_gate,
    expert_up,
    expert_down,
):
    mixed_out = mixer_half(queries, key_cache, value_cache, cum_gate, out_weight)
    expert_out = expert_half(
        routed_input, norm_gain, routes, route_weight, expert_gate, expert_up, expert_down
    )
    return (mixed_out, expert_out)


def solution(mesh):
    return jax.shard_map(
        body,
        mesh=mesh,
        in_specs=(
            P("ep", "tp"),
            P("tp", None, "ep"),
            P("tp", None, "ep"),
            P("tp", None),
            P(),
            P("ep", None),
            P(),
            P("ep", None),
            P("ep", None),
            P("ep", None, "tp"),
            P("ep", None, "tp"),
            P("ep", "tp", None),
        ),
        out_specs=(P(("ep", "tp"), None), P(("ep", "tp"), None)),
        check_vma=False,
    )
```

```python
import jax
import jax.numpy as jnp
from jax import lax
from jax.experimental import pallas as pl
from jax.experimental.pallas import tpu as pltpu
from jax.sharding import PartitionSpec as P

MESH = pl.DeviceIdType.MESH
BF = jnp.bfloat16
F32 = jnp.float32

D = 2048
ROWS = 64
CAP = 3
NT = 4
NZ = 8
NYC = 8
NE = NZ * NYC
SL = NE * CAP
TR = D // 128
CH = CAP * TR
QR = NYC * CH
ALL = NE * CH
NP = NZ // 2
PT = 2 * NYC * CAP
HID = 256
NY = 4
HEAD = 64
SEQ = 128
MIX = SEQ // NT
DZ = (0, 1, 7, 2, 6, 3, 5, 4)


def permutation():
    a = lax.broadcasted_iota(jnp.int32, (256, 256), 0)
    b = lax.broadcasted_iota(jnp.int32, (256, 256), 1)
    hit = ((a & 15) == (b >> 4)) & ((a >> 4) == (b & 15))
    return hit.astype(F32).astype(BF)


def mm(a, b):
    return jnp.dot(a, b, preferred_element_type=F32)


def rows_to_tiles(perm, src, row, dst, at):
    z = jnp.concatenate([src[row : row + 16, 128 * i : 128 * i + 128] for i in range(TR)], axis=0)
    dst[at : at + 256, :] = mm(perm, z).astype(BF)


def layer_kernel(
    x_hbm, routes_ref, rw_ref, gain_ref, wg_hbm, wu_hbm, wd_hbm, q_ref, key_hbm, value_hbm, gate_ref, wo_hbm,
    out_ref, mix_ref,
    xin, obuf, pick, send, recv, wg, wu, wd, xb, part, rs1, rss, rsd, sumb, tot, ret, back, resb, kv, wo, att, att_all,
    ld_sem, as_sem, a_sem, xs_sem, gl_sem, gr_sem, g2_sem, rr_sem, r1_sem, rss_sem, rsd_sem, bs_sem, b_sem,
    ks_sem, ku_sem, kd_sem, yu_sem, yd_sem, pc_sem, ts_sem, t_sem,
):
    t = lax.axis_index("tp")
    me = lax.axis_index("ep")
    z = me // NYC
    yc = me % NYC
    y = yc // 2
    c = yc % 2
    right = (t + 1) % NT
    left = (t + 3) % NT
    opp = (t + 2) % NT

    loads = [
        pltpu.make_async_copy(x_hbm.at[pl.ds(pl.multiple_of(t * ROWS, ROWS), ROWS), :], xin, ld_sem.at[0]),
        pltpu.make_async_copy(wg_hbm, wg, ld_sem.at[1]),
        pltpu.make_async_copy(wu_hbm, wu, ld_sem.at[2]),
        pltpu.make_async_copy(wd_hbm, wd, ld_sem.at[3]),
        pltpu.make_async_copy(wo_hbm, wo, ld_sem.at[4]),
        pltpu.make_async_copy(key_hbm, kv.at[z, y, c, pl.ds(0, HEAD), :], ld_sem.at[5]),
        pltpu.make_async_copy(value_hbm, kv.at[z, y, c, pl.ds(HEAD, HEAD), :], ld_sem.at[6]),
    ]
    for load in loads:
        load.start()

    barrier = pltpu.get_barrier_semaphore()

    def greet(k, _):
        pl.semaphore_signal(barrier, inc=1, device_id=((me + k) % NE, t), device_id_type=MESH)
        return 0

    lax.fori_loop(1, NE, greet, 0)
    for x in (right, left, opp):
        pl.semaphore_signal(barrier, inc=1, device_id=(me, x), device_id_type=MESH)

    perm = permutation()

    def kv_send(block, sem, to, way=0):
        return pltpu.make_async_remote_copy(
            src_ref=block, dst_ref=block, send_sem=ks_sem.at[way], recv_sem=sem, device_id=(to, t), device_id_type=MESH
        )

    def at_z(dz):
        return ((z + dz + NZ) % NZ) * NYC + yc

    def at_y(dy):
        return z * NYC + ((y + dy + NY) % NY) * 2 + c

    def kv_up(d):
        block = kv.at[(z + NZ - d) % NZ, y, c]
        if d > 0:
            kv_send(block, ku_sem.at[d - 1], at_z(1)).wait_recv()
        if d < NZ // 2:
            kv_send(block, ku_sem.at[d], at_z(1)).start()

    def kv_down(d):
        block = kv.at[(z + d) % NZ, y, c]
        if d > 0:
            kv_send(block, kd_sem.at[d - 1], at_z(-1)).wait_recv()
        if d < NZ // 2 - 1:
            kv_send(block, kd_sem.at[d], at_z(-1)).start()

    def column(dy):
        return kv.at[:, (y + dy + NY) % NY, c]

    def half(dy, up):
        return kv.at[pl.ds(0 if up else NZ // 2, NZ // 2), (y + dy + NY) % NY, c]

    partner = z * NYC + y * 2 + 1 - c

    def kv_rows(step):
        if step == 0:
            kv_send(column(0), yu_sem.at[0], at_y(1), 1).start()
            kv_send(column(0), yd_sem.at[0], at_y(-1), 1).start()
            kv_send(column(0), pc_sem.at[0], partner, 2).start()
        elif step == 1:
            kv_send(column(-1), yu_sem.at[0], at_y(1), 1).wait_recv()
            kv_send(half(-1, True), yu_sem.at[1], at_y(1), 1).start()
            kv_send(column(-1), pc_sem.at[1], partner, 2).start()
            kv_send(column(1), yd_sem.at[0], at_y(-1), 1).wait_recv()
            kv_send(half(1, False), yd_sem.at[1], at_y(-1), 1).start()
            kv_send(column(1), pc_sem.at[2], partner, 2).start()
        elif step == 2:
            kv_send(half(2, True), yu_sem.at[1], at_y(1), 1).wait_recv()
            kv_send(half(2, False), yd_sem.at[1], at_y(-1), 1).wait_recv()
            kv_send(column(2), pc_sem.at[3], partner, 2).start()
        else:
            for k, dy in enumerate((0, -1, 1, 2)):
                other = kv.at[:, (y + dy + NY) % NY, 1 - c]
                kv_send(other, pc_sem.at[k], partner, 2).wait_recv()

    def kv_step(d):
        kv_up(d)
        if d < NZ // 2:
            kv_down(d)

    def attend(_):
        lane = lax.broadcasted_iota(jnp.int32, (SEQ, 2 * HEAD), 1)
        q = q_ref[...].astype(F32) * (HEAD**-0.5)
        q = jnp.concatenate([jnp.where(lane < HEAD, q, 0.0), jnp.where(lane < HEAD, 0.0, q)], axis=0).astype(BF)
        own_gate = gate_ref[0:1, pl.ds(pl.multiple_of(me * SEQ, SEQ), SEQ)]
        column_gate = jnp.transpose(jnp.broadcast_to(own_gate, (SEQ, SEQ)))[:, 0:1]
        gq = jnp.concatenate([column_gate, column_gate], axis=0)
        wide = NYC * SEQ

        def scored(plane):
            keys = []
            for k in range(NYC):
                block = kv[plane, k // 2, k % 2, 0:HEAD, :]
                keys.append(jnp.concatenate([block, block], axis=0))
            gk = gate_ref[0:1, pl.ds(pl.multiple_of(plane * wide, wide), wide)]
            return mm(q, jnp.concatenate(keys, axis=1)) + (gq - gk)

        def folded(w):
            total = w[:, 0:SEQ]
            for k in range(1, NYC):
                total = total + w[:, k * SEQ : (k + 1) * SEQ]
            return total

        def mixed(plane, w):
            values = []
            for k in range(NYC):
                block = kv[plane, k // 2, k % 2, HEAD : 2 * HEAD, :]
                values.append(jnp.concatenate([block, block], axis=0))
            return lax.dot_general(
                w.astype(BF), jnp.concatenate(values, axis=1), (((1,), (1,)), ((), ())), preferred_element_type=F32
            )

        rows = lax.broadcasted_iota(jnp.int32, (2 * SEQ, wide), 0) & (SEQ - 1)
        cols = lax.broadcasted_iota(jnp.int32, (2 * SEQ, wide), 1)
        s = jnp.where(cols <= rows + yc * SEQ, scored(z), -jnp.inf)
        best = jnp.max(s, axis=1, keepdims=True)
        w = jnp.exp(s - best)

        def plane_step(plane, state):
            best, total, summed = state
            s = scored(plane)
            new = jnp.maximum(best, jnp.max(s, axis=1, keepdims=True))
            factor = jnp.exp(best - new)
            w = jnp.exp(s - new)
            return new, total * factor + folded(w), summed * factor + mixed(plane, w)

        best, total, summed = lax.fori_loop(0, z, plane_step, (best, folded(w), mixed(z, w)))
        result = summed / jnp.sum(total, axis=1, keepdims=True)
        result = jnp.where(lane < HEAD, result[0:SEQ, :], result[SEQ : 2 * SEQ, :])
        att[...] = result.astype(BF)
        for k, x in enumerate((right, left, opp)):
            att_send(k, x).start()
        att_all[t] = att[pl.ds(pl.multiple_of(t * MIX, MIX), MIX), :]

    def att_send(k, x):
        return pltpu.make_async_remote_copy(
            src_ref=att.at[pl.ds(pl.multiple_of(x * MIX, MIX), MIX), :], dst_ref=att_all.at[t],
            send_sem=ts_sem, recv_sem=t_sem.at[k], device_id=(me, x), device_id_type=MESH,
        )

    def project(_):
        for k, x in enumerate((left, right, opp)):
            pltpu.make_async_remote_copy(
                src_ref=att_all.at[x], dst_ref=att_all.at[x], send_sem=ts_sem, recv_sem=t_sem.at[k],
                device_id=(me, x), device_id_type=MESH,
            ).wait_recv()
        loads[4].wait()
        joined = jnp.concatenate([att_all[k] for k in range(NT)], axis=1)
        mix_ref[...] = mm(joined, wo[...]).astype(BF)

    own = pl.ds(pl.multiple_of(t * ROWS, ROWS), ROWS)
    r = routes_ref[own, :]
    r0 = r[:, 0:1]
    r1 = r[:, 1:2]
    lane = lax.broadcasted_iota(jnp.int32, (ROWS, NE), 1)
    s0 = jnp.where(r0 == lane, 1.0, 0.0)
    s1 = jnp.where(r1 == lane, 1.0, 0.0)
    low = jnp.where(
        lax.broadcasted_iota(jnp.int32, (ROWS, ROWS), 0) > lax.broadcasted_iota(jnp.int32, (ROWS, ROWS), 1), 1.0, 0.0
    )
    before = mm(low.astype(BF), (s0 + s1).astype(BF))
    k0 = jnp.sum(before * s0, axis=1, keepdims=True)
    k1 = jnp.sum((before + s0) * s1, axis=1, keepdims=True)
    slots = lax.broadcasted_iota(jnp.int32, (ROWS, SL), 1).astype(F32)
    c0 = jnp.where(r0.astype(F32) * CAP + k0 == slots, 1.0, 0.0)
    c1 = jnp.where(r1.astype(F32) * CAP + k1 == slots, 1.0, 0.0)
    pick[0:ROWS, :] = c0.astype(BF)
    pick[ROWS : 2 * ROWS, :] = c1.astype(BF)

    loads[0].wait()
    wide = xin[...].astype(F32)
    scale = lax.rsqrt(jnp.mean(wide * wide, axis=-1, keepdims=True) + 1e-06)
    normed = (wide * scale * gain_ref[...].astype(F32)).astype(BF)
    chosen = jnp.transpose(c0 + c1).astype(BF)
    obuf[...] = mm(chosen, normed).astype(BF)
    for g in range(SL // 16):
        rows_to_tiles(perm, obuf, 16 * g, send, 256 * g)

    loads[5].wait()
    loads[6].wait()
    pl.semaphore_wait(barrier, NE - 1 + 3)
    kv_up(0)
    kv_down(0)

    for q in range(NZ):
        far = ((z + DZ[q]) % NZ) * NYC

        def ship(j, _, q=q, far=far):
            to = far + (yc + j) % NYC
            pltpu.make_async_remote_copy(
                src_ref=send.at[pl.ds(pl.multiple_of(to * CH, CH), CH), :],
                dst_ref=recv.at[t, pl.ds(pl.multiple_of(q * QR + yc * CH, CH), CH), :],
                send_sem=as_sem,
                recv_sem=a_sem.at[q],
                device_id=(to, t),
                device_id_type=MESH,
            ).start()
            return 0

        lax.fori_loop(1 if q == 0 else 0, NYC, ship, 0)
    recv[t, pl.ds(pl.multiple_of(yc * CH, CH), CH), :] = send[pl.ds(pl.multiple_of(me * CH, CH), CH), :]

    def chunk(src, q):
        return recv.at[src, pl.ds(q * QR, QR), :]

    def hop(src, q, sem, x):
        return pltpu.make_async_remote_copy(
            src_ref=chunk(src, q), dst_ref=chunk(src, q), send_sem=xs_sem, recv_sem=sem.at[q],
            device_id=(me, x), device_id_type=MESH,
        )

    def arrive(q):
        n = QR - CH if q == 0 else QR
        pltpu.make_async_remote_copy(
            src_ref=send.at[pl.ds(0, n), :], dst_ref=recv.at[t, pl.ds(q * QR, n), :],
            send_sem=as_sem, recv_sem=a_sem.at[q], device_id=(me, right), device_id_type=MESH,
        ).wait_recv()

    def spread(q):
        arrive(q)
        hop(t, q, gl_sem, right).start()
        hop(t, q, gr_sem, left).start()

    def relay(q):
        if q % 2 == 0:
            hop(left, q, gl_sem, right).wait_recv()
            hop(left, q, g2_sem, right).start()
        else:
            hop(right, q, gr_sem, left).wait_recv()
            hop(right, q, g2_sem, left).start()

    def gathered(q):
        if q % 2 == 0:
            hop(right, q, gr_sem, left).wait_recv()
        else:
            hop(left, q, gl_sem, right).wait_recv()
        hop(opp, q, g2_sem, right).wait_recv()

    def rsend(src, dst, sem, p, x):
        return pltpu.make_async_remote_copy(
            src_ref=src, dst_ref=dst.at[p], send_sem=rr_sem, recv_sem=sem.at[p], device_id=(me, x), device_id_type=MESH
        )

    def ways(p):
        return (right, left) if p % 2 == 0 else (left, right)

    def experts(p):
        gathered(2 * p)
        gathered(2 * p + 1)
        if p == 0:
            for load in loads[1:4]:
                load.wait()
        for tt in range(NT):
            for g in range(PT // 16):
                at = p * 2 * QR + g * 256
                y = mm(perm, recv[tt, at : at + 256, :]).astype(BF)
                row = tt * PT + 16 * g
                for i in range(TR):
                    xb[row : row + 16, 128 * i : 128 * i + 128] = y[16 * i : 16 * i + 16, :]
        x = xb[...]
        gate = mm(x, wg[...])
        up = mm(x, wu[...])
        hidden = (gate / (1.0 + jnp.exp(-gate)) * up).astype(BF)
        for tt in range(NT):
            part[p, tt] = mm(hidden[tt * PT : (tt + 1) * PT, :], wd[...]).astype(BF)
        fwd, bwd = ways(p)
        rsend(part.at[p, opp], rs1, r1_sem, p, fwd).start()
        rsend(part.at[p, bwd], rss, rss_sem, p, bwd).start()

    def middle(p):
        fwd, bwd = ways(p)
        rsend(part.at[p, opp], rs1, r1_sem, p, fwd).wait_recv()
        sumb[p] = (rs1[p].astype(F32) + part[p, fwd].astype(F32)).astype(BF)
        rsend(sumb.at[p], rsd, rsd_sem, p, fwd).start()

    def finish(p):
        fwd, bwd = ways(p)
        rsend(part.at[p, bwd], rss, rss_sem, p, bwd).wait_recv()
        rsend(sumb.at[p], rsd, rsd_sem, p, fwd).wait_recv()
        tot[...] = (part[p, t].astype(F32) + rss[p].astype(F32) + rsd[p].astype(F32)).astype(BF)
        for g in range(PT // 16):
            rows_to_tiles(perm, tot, 16 * g, ret, p * 2 * QR + 256 * g)
        for q in (2 * p, 2 * p + 1):
            far = ((z + NZ - DZ[q]) % NZ) * NYC

            def home(j, _, q=q, far=far):
                to = (yc + j) % NYC
                pltpu.make_async_remote_copy(
                    src_ref=ret.at[pl.ds(pl.multiple_of(q * QR + to * CH, CH), CH), :],
                    dst_ref=back.at[pl.ds(pl.multiple_of(me * CH, CH), CH), :],
                    send_sem=bs_sem,
                    recv_sem=b_sem,
                    device_id=(far + to, t),
                    device_id_type=MESH,
                ).start()
                return 0

            lax.fori_loop(1 if q == 0 else 0, NYC, home, 0)
        if p == 0:
            back[pl.ds(pl.multiple_of(me * CH, CH), CH), :] = ret[pl.ds(pl.multiple_of(yc * CH, CH), CH), :]

    for step in (
        (spread, 0), (kv_step, 1), (spread, 1), (relay, 0), (kv_step, 2), (spread, 2), (relay, 1), (kv_step, 3),
        (spread, 3), (relay, 2), (kv_step, 4), (kv_rows, 0), (experts, 0),
        (spread, 4), (relay, 3), (kv_rows, 1), (spread, 5), (relay, 4), (kv_rows, 2), (experts, 1), (spread, 6),
        (relay, 5), (spread, 7), (relay, 6), (relay, 7), (middle, 0), (kv_rows, 3), (attend, 0),
        (experts, 2), (middle, 1), (finish, 0), (experts, 3), (middle, 2),
        (finish, 1), (project, 0), (middle, 3), (finish, 2), (finish, 3),
    ):
        step[0](step[1])

    n = ALL - CH
    last = pltpu.make_async_remote_copy(
        src_ref=ret.at[pl.ds(0, n), :], dst_ref=back.at[pl.ds(0, n), :], send_sem=bs_sem, recv_sem=b_sem,
        device_id=(me, right), device_id_type=MESH,
    )
    last.wait_recv()
    for g in range(SL // 16):
        y = mm(perm, back[256 * g : 256 * g + 256, :]).astype(BF)
        for i in range(TR):
            resb[16 * g : 16 * g + 16, 128 * i : 128 * i + 128] = y[16 * i : 16 * i + 16, :]
    picked = mm(pick[...], resb[...])
    w = rw_ref[own, :]
    out_ref[...] = (w[:, 0:1] * picked[0:ROWS, :] + w[:, 1:2] * picked[ROWS : 2 * ROWS, :]).astype(BF)

    last.wait_send()
    pltpu.make_async_remote_copy(
        src_ref=kv.at[:, pl.ds(0, 3), 0], dst_ref=kv.at[:, pl.ds(0, 3), 0], send_sem=ks_sem.at[1], recv_sem=ku_sem.at[0],
        device_id=(me, right), device_id_type=MESH,
    ).wait_send()
    pltpu.make_async_remote_copy(
        src_ref=kv.at[:, :, 0], dst_ref=kv.at[:, :, 0], send_sem=ks_sem.at[2], recv_sem=ku_sem.at[0],
        device_id=(me, right), device_id_type=MESH,
    ).wait_send()
    pltpu.make_async_remote_copy(
        src_ref=kv.at[pl.ds(0, NZ - 1), 0, 0], dst_ref=kv.at[pl.ds(0, NZ - 1), 0, 0], send_sem=ks_sem.at[0],
        recv_sem=ku_sem.at[0], device_id=(me, right), device_id_type=MESH,
    ).wait_send()
    pltpu.make_async_remote_copy(
        src_ref=att.at[pl.ds(0, 3 * MIX), :], dst_ref=att.at[pl.ds(0, 3 * MIX), :], send_sem=ts_sem,
        recv_sem=t_sem.at[0], device_id=(me, right), device_id_type=MESH,
    ).wait_send()
    pltpu.make_async_remote_copy(
        src_ref=send.at[pl.ds(0, n), :], dst_ref=recv.at[t, pl.ds(0, n), :], send_sem=as_sem, recv_sem=a_sem.at[0],
        device_id=(me, right), device_id_type=MESH,
    ).wait_send()
    pltpu.make_async_remote_copy(
        src_ref=recv.at[pl.ds(0, 3)], dst_ref=recv.at[pl.ds(0, 3)], send_sem=xs_sem, recv_sem=gl_sem.at[0],
        device_id=(me, right), device_id_type=MESH,
    ).wait_send()
    pltpu.make_async_remote_copy(
        src_ref=part.at[:, pl.ds(0, 3)], dst_ref=part.at[:, pl.ds(0, 3)], send_sem=rr_sem, recv_sem=r1_sem.at[0],
        device_id=(me, right), device_id_type=MESH,
    ).wait_send()


def body(
    queries,
    key_cache,
    value_cache,
    cum_gate,
    out_weight,
    routed_input,
    norm_gain,
    routes,
    route_weight,
    expert_gate,
    expert_up,
    expert_down,
):
    vmem = pl.BlockSpec(memory_space=pltpu.VMEM)
    hbm = pl.BlockSpec(memory_space=pl.ANY)
    dma = pltpu.SemaphoreType.DMA
    expert_out, mixed_out = pl.pallas_call(
        layer_kernel,
        out_shape=(jax.ShapeDtypeStruct((ROWS, D), BF), jax.ShapeDtypeStruct((MIX, D), BF)),
        in_specs=[hbm, vmem, vmem, vmem, hbm, hbm, hbm, vmem, hbm, hbm, vmem, hbm],
        out_specs=(vmem, vmem),
        scratch_shapes=[
            pltpu.VMEM((ROWS, D), BF),
            pltpu.VMEM((SL, D), BF),
            pltpu.VMEM((2 * ROWS, SL), BF),
            pltpu.VMEM((ALL, 128), BF),
            pltpu.VMEM((NT, ALL, 128), BF),
            pltpu.VMEM((D, HID), BF),
            pltpu.VMEM((D, HID), BF),
            pltpu.VMEM((HID, D), BF),
            pltpu.VMEM((NT * PT, D), BF),
            pltpu.VMEM((NP, NT, PT, D), BF),
            pltpu.VMEM((NP, PT, D), BF),
            pltpu.VMEM((NP, PT, D), BF),
            pltpu.VMEM((NP, PT, D), BF),
            pltpu.VMEM((NP, PT, D), BF),
            pltpu.VMEM((PT, D), BF),
            pltpu.VMEM((ALL, 128), BF),
            pltpu.VMEM((ALL, 128), BF),
            pltpu.VMEM((SL, D), BF),
            pltpu.VMEM((NZ, NY, 2, 2 * HEAD, SEQ), BF),
            pltpu.VMEM((NT * 2 * HEAD, D), BF),
            pltpu.VMEM((SEQ, 2 * HEAD), BF),
            pltpu.VMEM((NT, MIX, 2 * HEAD), BF),
            dma((7,)),
            dma,
            dma((NZ,)),
            dma,
            dma((NZ,)),
            dma((NZ,)),
            dma((NZ,)),
            dma,
            dma((NP,)),
            dma((NP,)),
            dma((NP,)),
            dma,
            dma,
            dma((3,)),
            dma((4,)),
            dma((3,)),
            dma((2,)),
            dma((2,)),
            dma((4,)),
            dma,
            dma((3,)),
        ],
        compiler_params=pltpu.CompilerParams(collective_id=0, has_side_effects=True, vmem_limit_bytes=67043328),
        cost_estimate=pl.CostEstimate(flops=60_000_000_000, bytes_accessed=8_000_000, transcendentals=0),
        name="layer",
    )(
        routed_input, routes, route_weight, norm_gain.reshape(1, D),
        expert_gate[0], expert_up[0], expert_down[0],
        queries, key_cache[0], value_cache[0], cum_gate, out_weight,
    )
    return (mixed_out, expert_out)


def solution(mesh):
    return jax.shard_map(
        body,
        mesh=mesh,
        in_specs=(
            P("ep", "tp"),
            P("tp", None, "ep"),
            P("tp", None, "ep"),
            P("tp", None),
            P(),
            P("ep", None),
            P(),
            P("ep", None),
            P("ep", None),
            P("ep", None, "tp"),
            P("ep", None, "tp"),
            P("ep", "tp", None),
        ),
        out_specs=(P(("ep", "tp"), None), P(("ep", "tp"), None)),
        check_vma=False,
    )
```

```python
import jax
import jax.numpy as jnp
from jax import lax
from jax.experimental import pallas as pl
from jax.experimental.pallas import tpu as pltpu
from jax.sharding import PartitionSpec as P

MESH = pl.DeviceIdType.MESH
BF = jnp.bfloat16
F32 = jnp.float32

D = 2048
ROWS = 64
CAP = 3
NT = 4
NZ = 8
NYC = 8
NE = NZ * NYC
SL = NE * CAP
TR = D // 128
CH = CAP * TR
QR = NYC * CH
ALL = NE * CH
NP = NZ // 2
PT = 2 * NYC * CAP
HID = 256
NY = 4
HEAD = 64
SEQ = 128
MIX = SEQ // NT
DZ = (0, 7, 2, 1, 3, 5, 6, 4)
ORDER = (
    ("spread", 0), ("spread", 1), ("relay", 0), ("spread", 2), ("spread", 3), ("spread", 5),
    ("relay", 1), ("spread", 6), ("spread", 4), ("relay", 2), ("kv", 0), ("relay", 5),
    ("relay", 4), ("spread", 7), ("relay", 3), ("kv", 1), ("relay", 6), ("kv", 2),
    ("relay", 7), ("experts", 2), ("kv", 3), ("experts", 3), ("kv", 4), ("rows", 0),
    ("middle", 2), ("experts", 1), ("middle", 3), ("finish", 2), ("middle", 1), ("rows", 1),
    ("experts", 0), ("finish", 3), ("rows", 2), ("middle", 0), ("rows", 3), ("finish", 1),
    ("attend", 0), ("finish", 0), ("project", 0),
)


def permutation():
    a = lax.broadcasted_iota(jnp.int32, (256, 256), 0)
    b = lax.broadcasted_iota(jnp.int32, (256, 256), 1)
    hit = ((a & 15) == (b >> 4)) & ((a >> 4) == (b & 15))
    return hit.astype(F32).astype(BF)


def mm(a, b):
    return jnp.dot(a, b, preferred_element_type=F32)


def rows_to_tiles(perm, src, row, dst, at):
    z = jnp.concatenate([src[row : row + 16, 128 * i : 128 * i + 128] for i in range(TR)], axis=0)
    dst[at : at + 256, :] = mm(perm, z).astype(BF)


def layer_kernel(
    x_ref, routes_ref, rw_ref, gain_ref, wg_hbm, wu_hbm, wd_hbm, q_ref, key_hbm, value_hbm, gate_ref, wo_hbm,
    out_ref, mix_ref,
    xin, obuf, pick, wcol, send, recv, wg, wu, wd, xb, part, rs1, rss, rsd, sumb, tot, ret, back, resb, kv, wo, att, att_all,
    ld_sem, as_sem, a_sem, xs_sem, gl_sem, gr_sem, g2_sem, rr_sem, r1_sem, rss_sem, rsd_sem, bs_sem, b_sem,
    ks_sem, ku_sem, kd_sem, yu_sem, yd_sem, pc_sem, ts_sem, t_sem,
):
    t = lax.axis_index("tp")
    me = lax.axis_index("ep")
    z = me // NYC
    yc = me % NYC
    y = yc // 2
    c = yc % 2
    right = (t + 1) % NT
    left = (t + 3) % NT
    opp = (t + 2) % NT

    loads = [
        pltpu.make_async_copy(x_ref.at[pl.ds(pl.multiple_of(t * ROWS, ROWS), ROWS), :], xin, ld_sem.at[0]),
        pltpu.make_async_copy(wg_hbm, wg, ld_sem.at[1]),
        pltpu.make_async_copy(wu_hbm, wu, ld_sem.at[2]),
        pltpu.make_async_copy(wd_hbm, wd, ld_sem.at[3]),
        pltpu.make_async_copy(wo_hbm, wo, ld_sem.at[4]),
        pltpu.make_async_copy(key_hbm, kv.at[z, y, c, pl.ds(0, HEAD), :], ld_sem.at[5]),
        pltpu.make_async_copy(value_hbm, kv.at[z, y, c, pl.ds(HEAD, HEAD), :], ld_sem.at[6]),
    ]
    for load in loads:
        load.start()

    barrier = pltpu.get_barrier_semaphore()

    def greet(k, _):
        pl.semaphore_signal(barrier, inc=1, device_id=((me + k) % NE, t), device_id_type=MESH)
        return 0

    lax.fori_loop(1, NE, greet, 0)
    for x in (right, left, opp):
        pl.semaphore_signal(barrier, inc=1, device_id=(me, x), device_id_type=MESH)

    perm = permutation()

    def kv_send(block, sem, to, way=0):
        return pltpu.make_async_remote_copy(
            src_ref=block, dst_ref=block, send_sem=ks_sem.at[way], recv_sem=sem, device_id=(to, t), device_id_type=MESH
        )

    def at_z(dz):
        return ((z + dz + NZ) % NZ) * NYC + yc

    def at_y(dy):
        return z * NYC + ((y + dy + NY) % NY) * 2 + c

    def kv_up(d):
        block = kv.at[(z + NZ - d) % NZ, y, c]
        if d > 0:
            kv_send(block, ku_sem.at[d - 1], at_z(1)).wait_recv()
        if d < NZ // 2:
            kv_send(block, ku_sem.at[d], at_z(1)).start()

    def kv_down(d):
        block = kv.at[(z + d) % NZ, y, c]
        if d > 0:
            kv_send(block, kd_sem.at[d - 1], at_z(-1)).wait_recv()
        if d < NZ // 2 - 1:
            kv_send(block, kd_sem.at[d], at_z(-1)).start()

    def column(dy):
        return kv.at[:, (y + dy + NY) % NY, c]

    def half(dy, up):
        return kv.at[pl.ds(0 if up else NZ // 2, NZ // 2), (y + dy + NY) % NY, c]

    partner = z * NYC + y * 2 + 1 - c

    def kv_rows(step):
        if step == 0:
            kv_send(column(0), yu_sem.at[0], at_y(1), 1).start()
            kv_send(column(0), yd_sem.at[0], at_y(-1), 1).start()
            kv_send(column(0), pc_sem.at[0], partner, 2).start()
        elif step == 1:
            kv_send(column(-1), yu_sem.at[0], at_y(1), 1).wait_recv()
            kv_send(half(-1, True), yu_sem.at[1], at_y(1), 1).start()
            kv_send(column(-1), pc_sem.at[1], partner, 2).start()
            kv_send(column(1), yd_sem.at[0], at_y(-1), 1).wait_recv()
            kv_send(half(1, False), yd_sem.at[1], at_y(-1), 1).start()
            kv_send(column(1), pc_sem.at[2], partner, 2).start()
        elif step == 2:
            kv_send(half(2, True), yu_sem.at[1], at_y(1), 1).wait_recv()
            kv_send(half(2, False), yd_sem.at[1], at_y(-1), 1).wait_recv()
            kv_send(column(2), pc_sem.at[3], partner, 2).start()
        else:
            for k, dy in enumerate((0, -1, 1, 2)):
                other = kv.at[:, (y + dy + NY) % NY, 1 - c]
                kv_send(other, pc_sem.at[k], partner, 2).wait_recv()

    def kv_step(d):
        kv_up(d)
        if d < NZ // 2:
            kv_down(d)

    def attend(_):
        lane = lax.broadcasted_iota(jnp.int32, (SEQ, 2 * HEAD), 1)
        q = q_ref[...].astype(F32) * (HEAD**-0.5)
        q = jnp.concatenate([jnp.where(lane < HEAD, q, 0.0), jnp.where(lane < HEAD, 0.0, q)], axis=0).astype(BF)
        own_gate = gate_ref[0:1, pl.ds(pl.multiple_of(me * SEQ, SEQ), SEQ)]
        column_gate = jnp.transpose(jnp.broadcast_to(own_gate, (SEQ, SEQ)))[:, 0:1]
        gq = jnp.concatenate([column_gate, column_gate], axis=0)
        wide = NYC * SEQ

        def scored(plane):
            keys = []
            for k in range(NYC):
                block = kv[plane, k // 2, k % 2, 0:HEAD, :]
                keys.append(jnp.concatenate([block, block], axis=0))
            gk = gate_ref[0:1, pl.ds(pl.multiple_of(plane * wide, wide), wide)]
            return mm(q, jnp.concatenate(keys, axis=1)) + (gq - gk)

        def folded(w):
            total = w[:, 0:SEQ]
            for k in range(1, NYC):
                total = total + w[:, k * SEQ : (k + 1) * SEQ]
            return total

        def mixed(plane, w):
            values = []
            for k in range(NYC):
                block = kv[plane, k // 2, k % 2, HEAD : 2 * HEAD, :]
                values.append(jnp.concatenate([block, block], axis=0))
            return lax.dot_general(
                w.astype(BF), jnp.concatenate(values, axis=1), (((1,), (1,)), ((), ())), preferred_element_type=F32
            )

        rows = lax.broadcasted_iota(jnp.int32, (2 * SEQ, wide), 0) & (SEQ - 1)
        cols = lax.broadcasted_iota(jnp.int32, (2 * SEQ, wide), 1)
        s = jnp.where(cols <= rows + yc * SEQ, scored(z), -jnp.inf)
        best = jnp.max(s, axis=1, keepdims=True)
        w = jnp.exp(s - best)

        def plane_step(plane, state):
            best, total, summed = state
            s = scored(plane)
            new = jnp.maximum(best, jnp.max(s, axis=1, keepdims=True))
            factor = jnp.exp(best - new)
            w = jnp.exp(s - new)
            return new, total * factor + folded(w), summed * factor + mixed(plane, w)

        best, total, summed = lax.fori_loop(0, z, plane_step, (best, folded(w), mixed(z, w)))
        result = summed / jnp.sum(total, axis=1, keepdims=True)
        result = jnp.where(lane < HEAD, result[0:SEQ, :], result[SEQ : 2 * SEQ, :])
        att[...] = result.astype(BF)
        for k, x in enumerate((right, left, opp)):
            att_send(k, x).start()
        att_all[t] = att[pl.ds(pl.multiple_of(t * MIX, MIX), MIX), :]

    def att_send(k, x):
        return pltpu.make_async_remote_copy(
            src_ref=att.at[pl.ds(pl.multiple_of(x * MIX, MIX), MIX), :], dst_ref=att_all.at[t],
            send_sem=ts_sem, recv_sem=t_sem.at[k], device_id=(me, x), device_id_type=MESH,
        )

    def project(_):
        for k, x in enumerate((left, right, opp)):
            pltpu.make_async_remote_copy(
                src_ref=att_all.at[x], dst_ref=att_all.at[x], send_sem=ts_sem, recv_sem=t_sem.at[k],
                device_id=(me, x), device_id_type=MESH,
            ).wait_recv()
        loads[4].wait()
        joined = jnp.concatenate([att_all[k] for k in range(NT)], axis=1)
        mix_ref[...] = mm(joined, wo[...]).astype(BF)

    own = pl.ds(pl.multiple_of(t * ROWS, ROWS), ROWS)
    tokens = NT * ROWS
    r = routes_ref[...]
    r0 = r[0:1, :]
    r1 = r[1:2, :]
    expert = lax.broadcasted_iota(jnp.int32, (NE, tokens), 0)
    s0 = jnp.where(r0 == expert, 1.0, 0.0)
    s1 = jnp.where(r1 == expert, 1.0, 0.0)
    ta = lax.broadcasted_iota(jnp.int32, (tokens, tokens), 0)
    tb = lax.broadcasted_iota(jnp.int32, (tokens, tokens), 1)
    earlier = jnp.where((ta < tb) & ((ta >> 6) == (tb >> 6)), 1.0, 0.0).astype(BF)
    before = mm((s0 + s1).astype(BF), earlier)
    slot0 = r0.astype(F32) * CAP + jnp.sum(before * s0, axis=0, keepdims=True)
    slot1 = r1.astype(F32) * CAP + jnp.sum((before + s0) * s1, axis=0, keepdims=True)

    slot = lax.broadcasted_iota(jnp.int32, (SL, tokens), 0).astype(F32)
    pick[0:tokens, :] = jnp.transpose(jnp.where(slot0 == slot, 1.0, 0.0)).astype(BF)
    pick[tokens : 2 * tokens, :] = jnp.transpose(jnp.where(slot1 == slot, 1.0, 0.0)).astype(BF)
    wcol[...] = jnp.transpose(jnp.concatenate([rw_ref[...], jnp.zeros((6, tokens), F32)], axis=0))
    both = jnp.concatenate([pick[own, :], pick[pl.ds(pl.multiple_of(tokens + t * ROWS, ROWS), ROWS), :]], axis=0)

    loads[0].wait()
    wide = xin[...].astype(F32)
    scale = lax.rsqrt(jnp.mean(wide * wide, axis=-1, keepdims=True) + 1e-06)
    normed = (wide * scale * gain_ref[...].astype(F32)[None, :]).astype(BF)
    chosen = jnp.transpose(both[0:ROWS, :].astype(F32) + both[ROWS : 2 * ROWS, :].astype(F32)).astype(BF)
    obuf[...] = mm(chosen, normed).astype(BF)
    for g in range(SL // 16):
        rows_to_tiles(perm, obuf, 16 * g, send, 256 * g)

    loads[5].wait()
    loads[6].wait()
    pl.semaphore_wait(barrier, NE - 1 + 3)

    for q in range(NZ):
        far = ((z + DZ[q]) % NZ) * NYC

        def ship(j, _, q=q, far=far):
            to = far + (yc + j) % NYC
            src = send.at[pl.ds(pl.multiple_of(to * CH, CH), CH), :]
            dst = recv.at[t, pl.ds(pl.multiple_of(q * QR + yc * CH, CH), CH), :]
            pltpu.make_async_remote_copy(
                src_ref=src, dst_ref=dst, send_sem=as_sem, recv_sem=a_sem.at[q],
                device_id=(to, t), device_id_type=MESH,
            ).start()
            return 0

        lax.fori_loop(1 if q == 0 else 0, NYC, ship, 0)
    recv[t, pl.ds(pl.multiple_of(yc * CH, CH), CH), :] = send[pl.ds(pl.multiple_of(me * CH, CH), CH), :]

    def chunk(src, q):
        return recv.at[src, pl.ds(q * QR, QR), :]

    def hop(src, q, sem, x):
        return pltpu.make_async_remote_copy(
            src_ref=chunk(src, q), dst_ref=chunk(src, q), send_sem=xs_sem, recv_sem=sem.at[q],
            device_id=(me, x), device_id_type=MESH,
        )

    def arrive(q):
        n = QR - CH if q == 0 else QR
        dst = recv.at[t, pl.ds(q * QR, n), :]
        pltpu.make_async_remote_copy(
            src_ref=dst, dst_ref=dst,
            send_sem=as_sem, recv_sem=a_sem.at[q], device_id=(me, right), device_id_type=MESH,
        ).wait_recv()

    def spread(q):
        arrive(q)
        hop(t, q, gl_sem, right).start()
        hop(t, q, gr_sem, left).start()

    def relay(q):
        if q % 2 == 0:
            hop(left, q, gl_sem, right).wait_recv()
            hop(left, q, g2_sem, right).start()
        else:
            hop(right, q, gr_sem, left).wait_recv()
            hop(right, q, g2_sem, left).start()

    def gathered(q):
        if q % 2 == 0:
            hop(right, q, gr_sem, left).wait_recv()
        else:
            hop(left, q, gl_sem, right).wait_recv()
        hop(opp, q, g2_sem, right).wait_recv()

    def rsend(src, dst, sem, p, x):
        return pltpu.make_async_remote_copy(
            src_ref=src, dst_ref=dst.at[p], send_sem=rr_sem, recv_sem=sem.at[p], device_id=(me, x), device_id_type=MESH
        )

    def ways(p):
        return (right, left) if p % 2 == 0 else (left, right)

    first = next(step for step in ORDER if step[0] == "experts")

    def experts(p):
        gathered(2 * p)
        gathered(2 * p + 1)
        if ("experts", p) == first:
            for load in loads[1:4]:
                load.wait()
        for tt in range(NT):
            for g in range(PT // 16):
                at = p * 2 * QR + g * 256
                y = mm(perm, recv[tt, at : at + 256, :]).astype(BF)
                row = tt * PT + 16 * g
                for i in range(TR):
                    xb[row : row + 16, 128 * i : 128 * i + 128] = y[16 * i : 16 * i + 16, :]
        x = xb[...]
        gate = mm(x, wg[...])
        up = mm(x, wu[...])
        hidden = (gate / (1.0 + jnp.exp(-gate)) * up).astype(BF)
        for tt in range(NT):
            part[p, tt] = mm(hidden[tt * PT : (tt + 1) * PT, :], wd[...]).astype(BF)
        fwd, bwd = ways(p)
        rsend(part.at[p, opp], rs1, r1_sem, p, fwd).start()
        rsend(part.at[p, bwd], rss, rss_sem, p, bwd).start()

    def middle(p):
        fwd, bwd = ways(p)
        rsend(part.at[p, opp], rs1, r1_sem, p, fwd).wait_recv()
        sumb[p] = (rs1[p].astype(F32) + part[p, fwd].astype(F32)).astype(BF)
        rsend(sumb.at[p], rsd, rsd_sem, p, fwd).start()

    def finish(p):
        fwd, bwd = ways(p)
        rsend(part.at[p, bwd], rss, rss_sem, p, bwd).wait_recv()
        rsend(sumb.at[p], rsd, rsd_sem, p, fwd).wait_recv()
        tot[...] = (part[p, t].astype(F32) + rss[p].astype(F32) + rsd[p].astype(F32)).astype(BF)
        for g in range(PT // 16):
            rows_to_tiles(perm, tot, 16 * g, ret, p * 2 * QR + 256 * g)
        for q in (2 * p, 2 * p + 1):
            far = ((z + NZ - DZ[q]) % NZ) * NYC

            def home(j, _, q=q, far=far):
                to = (yc + j) % NYC
                pltpu.make_async_remote_copy(
                    src_ref=ret.at[pl.ds(pl.multiple_of(q * QR + to * CH, CH), CH), :],
                    dst_ref=back.at[pl.ds(pl.multiple_of(me * CH, CH), CH), :],
                    send_sem=bs_sem,
                    recv_sem=b_sem,
                    device_id=(far + to, t),
                    device_id_type=MESH,
                ).start()
                return 0

            lax.fori_loop(1 if q == 0 else 0, NYC, home, 0)
        if p == 0:
            back[pl.ds(pl.multiple_of(me * CH, CH), CH), :] = ret[pl.ds(pl.multiple_of(yc * CH, CH), CH), :]

    steps = dict(
        spread=spread, relay=relay, experts=experts, middle=middle, finish=finish, kv=kv_step, rows=kv_rows,
        attend=attend, project=project,
    )
    for name, index in ORDER:
        steps[name](index)

    n = ALL - CH
    last = pltpu.make_async_remote_copy(
        src_ref=ret.at[pl.ds(0, n), :], dst_ref=back.at[pl.ds(0, n), :], send_sem=bs_sem, recv_sem=b_sem,
        device_id=(me, right), device_id_type=MESH,
    )
    last.wait_recv()
    for g in range(SL // 16):
        y = mm(perm, back[256 * g : 256 * g + 256, :]).astype(BF)
        for i in range(TR):
            resb[16 * g : 16 * g + 16, 128 * i : 128 * i + 128] = y[16 * i : 16 * i + 16, :]
    picked = mm(both, resb[...])
    w = wcol[own, :]
    out_ref[...] = (w[:, 0:1] * picked[0:ROWS, :] + w[:, 1:2] * picked[ROWS : 2 * ROWS, :]).astype(BF)

    last.wait_send()
    pltpu.make_async_remote_copy(
        src_ref=kv.at[:, pl.ds(0, 3), 0], dst_ref=kv.at[:, pl.ds(0, 3), 0], send_sem=ks_sem.at[1], recv_sem=ku_sem.at[0],
        device_id=(me, right), device_id_type=MESH,
    ).wait_send()
    pltpu.make_async_remote_copy(
        src_ref=kv.at[:, :, 0], dst_ref=kv.at[:, :, 0], send_sem=ks_sem.at[2], recv_sem=ku_sem.at[0],
        device_id=(me, right), device_id_type=MESH,
    ).wait_send()
    pltpu.make_async_remote_copy(
        src_ref=kv.at[pl.ds(0, NZ - 1), 0, 0], dst_ref=kv.at[pl.ds(0, NZ - 1), 0, 0], send_sem=ks_sem.at[0],
        recv_sem=ku_sem.at[0], device_id=(me, right), device_id_type=MESH,
    ).wait_send()
    pltpu.make_async_remote_copy(
        src_ref=att.at[pl.ds(0, 3 * MIX), :], dst_ref=att.at[pl.ds(0, 3 * MIX), :], send_sem=ts_sem,
        recv_sem=t_sem.at[0], device_id=(me, right), device_id_type=MESH,
    ).wait_send()
    pltpu.make_async_remote_copy(
        src_ref=send.at[pl.ds(0, n), :], dst_ref=send.at[pl.ds(0, n), :], send_sem=as_sem, recv_sem=a_sem.at[0],
        device_id=(me, right), device_id_type=MESH,
    ).wait_send()
    pltpu.make_async_remote_copy(
        src_ref=recv.at[pl.ds(0, 3)], dst_ref=recv.at[pl.ds(0, 3)], send_sem=xs_sem, recv_sem=gl_sem.at[0],
        device_id=(me, right), device_id_type=MESH,
    ).wait_send()
    pltpu.make_async_remote_copy(
        src_ref=part.at[:, pl.ds(0, 3)], dst_ref=part.at[:, pl.ds(0, 3)], send_sem=rr_sem, recv_sem=r1_sem.at[0],
        device_id=(me, right), device_id_type=MESH,
    ).wait_send()


def body(
    queries,
    key_cache,
    value_cache,
    cum_gate,
    out_weight,
    routed_input,
    norm_gain,
    routes,
    route_weight,
    expert_gate,
    expert_up,
    expert_down,
):
    vmem = pl.BlockSpec(memory_space=pltpu.VMEM)
    hbm = pl.BlockSpec(memory_space=pl.ANY)
    dma = pltpu.SemaphoreType.DMA
    expert_out, mixed_out = pl.pallas_call(
        layer_kernel,
        out_shape=(jax.ShapeDtypeStruct((ROWS, D), BF), jax.ShapeDtypeStruct((MIX, D), BF)),
        in_specs=[hbm, vmem, vmem, vmem, hbm, hbm, hbm, vmem, hbm, hbm, vmem, hbm],
        out_specs=(vmem, vmem),
        scratch_shapes=[
            pltpu.VMEM((ROWS, D), BF),
            pltpu.VMEM((SL, D), BF),
            pltpu.VMEM((2 * NT * ROWS, SL), BF),
            pltpu.VMEM((NT * ROWS, 8), F32),
            pltpu.VMEM((ALL, 128), BF),
            pltpu.VMEM((NT, ALL, 128), BF),
            pltpu.VMEM((D, HID), BF),
            pltpu.VMEM((D, HID), BF),
            pltpu.VMEM((HID, D), BF),
            pltpu.VMEM((NT * PT, D), BF),
            pltpu.VMEM((NP, NT, PT, D), BF),
            pltpu.VMEM((NP, PT, D), BF),
            pltpu.VMEM((NP, PT, D), BF),
            pltpu.VMEM((NP, PT, D), BF),
            pltpu.VMEM((NP, PT, D), BF),
            pltpu.VMEM((PT, D), BF),
            pltpu.VMEM((ALL, 128), BF),
            pltpu.VMEM((ALL, 128), BF),
            pltpu.VMEM((SL, D), BF),
            pltpu.VMEM((NZ, NY, 2, 2 * HEAD, SEQ), BF),
            pltpu.VMEM((NT * 2 * HEAD, D), BF),
            pltpu.VMEM((SEQ, 2 * HEAD), BF),
            pltpu.VMEM((NT, MIX, 2 * HEAD), BF),
            dma((7,)),
            dma,
            dma((NZ,)),
            dma,
            dma((NZ,)),
            dma((NZ,)),
            dma((NZ,)),
            dma,
            dma((NP,)),
            dma((NP,)),
            dma((NP,)),
            dma,
            dma,
            dma((3,)),
            dma((4,)),
            dma((3,)),
            dma((2,)),
            dma((2,)),
            dma((4,)),
            dma,
            dma((3,)),
        ],
        compiler_params=pltpu.CompilerParams(collective_id=0, has_side_effects=True, vmem_limit_bytes=67043328),
        cost_estimate=pl.CostEstimate(flops=60_000_000_000, bytes_accessed=8_000_000, transcendentals=0),
        name="layer",
    )(
        routed_input, routes.T, route_weight.T, norm_gain,
        expert_gate[0], expert_up[0], expert_down[0],
        queries, key_cache[0], value_cache[0], cum_gate, out_weight,
    )
    return (mixed_out, expert_out)


def solution(mesh):
    return jax.shard_map(
        body,
        mesh=mesh,
        in_specs=(
            P("ep", "tp"),
            P("tp", None, "ep"),
            P("tp", None, "ep"),
            P("tp", None),
            P(),
            P("ep", None),
            P(),
            P("ep", None),
            P("ep", None),
            P("ep", None, "tp"),
            P("ep", None, "tp"),
            P("ep", "tp", None),
        ),
        out_specs=(P(("ep", "tp"), None), P(("ep", "tp"), None)),
        check_vma=False,
    )
```

```python
import jax
import jax.numpy as jnp
from jax import lax
from jax.experimental import pallas as pl
from jax.experimental.pallas import tpu as pltpu
from jax.sharding import PartitionSpec as P

MESH = pl.DeviceIdType.MESH
BF = jnp.bfloat16
F32 = jnp.float32

D = 2048
ROWS = 64
CAP = 3
NT = 4
NZ = 8
NYC = 8
NE = NZ * NYC
SL = NE * CAP
TR = D // 128
CH = CAP * TR
QR = NYC * CH
ALL = NE * CH
NP = NZ // 2
PT = 2 * NYC * CAP
HID = 256
NY = 4
HEAD = 64
SEQ = 128
MIX = SEQ // NT
DZ = (0, 1, 7, 2, 3, 6, 5, 4)
ISSUE = (4, 5, 0, 6, 3, 7, 2, 1)
FULL = tuple(q for q in range(NZ) if DZ[q] in (1, 7))
PARTS = tuple(q for q in range(NZ) if q not in FULL)
BLK = NYC * CAP
ORDER = (
    ("spread", 0), ("spread", 5), ("spread", 4), ("relay", 0), ("relay", 5), ("spread", 3),
    ("spread", 6), ("relay", 4), ("spread", 7), ("relay", 6), ("relay", 3), ("relay", 7),
    ("kv", 0), ("experts", 2), ("spread", 2), ("spread", 1), ("kv", 1), ("experts", 3),
    ("kv", 2), ("kv", 3), ("middle", 2), ("experts", 1), ("kv", 4), ("rows", 0),
    ("middle", 3), ("finish", 2), ("middle", 1), ("experts", 0), ("rows", 1), ("finish", 3),
    ("middle", 0), ("rows", 2), ("finish", 1), ("rows", 3), ("attend", 0), ("finish", 0),
    ("project", 0),
)


def permutation():
    a = lax.broadcasted_iota(jnp.int32, (256, 256), 0)
    b = lax.broadcasted_iota(jnp.int32, (256, 256), 1)
    hit = ((a & 15) == (b >> 4)) & ((a >> 4) == (b & 15))
    return hit.astype(F32).astype(BF)


def mm(a, b):
    return jnp.dot(a, b, preferred_element_type=F32)


def rows_to_tiles(perm, src, row, dst, at):
    z = jnp.concatenate([src[row : row + 16, 128 * i : 128 * i + 128] for i in range(TR)], axis=0)
    dst[at : at + 256, :] = mm(perm, z).astype(BF)


def layer_kernel(
    x_ref, routes_ref, rw_ref, gain_ref, wg_hbm, wu_hbm, wd_hbm, q_ref, key_hbm, value_hbm, gate_ref, wo_hbm,
    out_ref, mix_ref,
    xin, normed, obuf, pick, wcol, send, sendp, recv, wg, wu, wd, xb, part, rs1, rss, rsd, sumb, tot, ret, back, resb, kv, wo, att, att_all,
    ld_sem, as_sem, ap_sem, a_sem, xs_sem, gl_sem, gr_sem, g2_sem, rr_sem, r1_sem, rss_sem, rsd_sem, bs_sem, b_sem,
    ks_sem, ku_sem, kd_sem, yu_sem, yd_sem, pc_sem, ts_sem, t_sem,
):
    t = lax.axis_index("tp")
    me = lax.axis_index("ep")
    z = me // NYC
    yc = me % NYC
    y = yc // 2
    c = yc % 2
    right = (t + 1) % NT
    left = (t + 3) % NT
    opp = (t + 2) % NT

    loads = [
        pltpu.make_async_copy(x_ref, xin, ld_sem.at[0]),
        pltpu.make_async_copy(wg_hbm, wg, ld_sem.at[1]),
        pltpu.make_async_copy(wu_hbm, wu, ld_sem.at[2]),
        pltpu.make_async_copy(wd_hbm, wd, ld_sem.at[3]),
        pltpu.make_async_copy(wo_hbm, wo, ld_sem.at[4]),
        pltpu.make_async_copy(key_hbm, kv.at[z, y, c, pl.ds(0, HEAD), :], ld_sem.at[5]),
        pltpu.make_async_copy(value_hbm, kv.at[z, y, c, pl.ds(HEAD, HEAD), :], ld_sem.at[6]),
    ]
    for load in loads:
        load.start()

    barrier = pltpu.get_barrier_semaphore()

    def greet(k, _):
        pl.semaphore_signal(barrier, inc=1, device_id=((me + k) % NE, t), device_id_type=MESH)
        return 0

    lax.fori_loop(1, NE, greet, 0)
    for x in (right, left, opp):
        pl.semaphore_signal(barrier, inc=1, device_id=(me, x), device_id_type=MESH)

    perm = permutation()

    def kv_send(block, sem, to, way=0):
        return pltpu.make_async_remote_copy(
            src_ref=block, dst_ref=block, send_sem=ks_sem.at[way], recv_sem=sem, device_id=(to, t), device_id_type=MESH
        )

    def at_z(dz):
        return ((z + dz + NZ) % NZ) * NYC + yc

    def at_y(dy):
        return z * NYC + ((y + dy + NY) % NY) * 2 + c

    def kv_up(d):
        block = kv.at[(z + NZ - d) % NZ, y, c]
        if d > 0:
            kv_send(block, ku_sem.at[d - 1], at_z(1)).wait_recv()
        if d < NZ // 2:
            kv_send(block, ku_sem.at[d], at_z(1)).start()

    def kv_down(d):
        block = kv.at[(z + d) % NZ, y, c]
        if d > 0:
            kv_send(block, kd_sem.at[d - 1], at_z(-1)).wait_recv()
        if d < NZ // 2 - 1:
            kv_send(block, kd_sem.at[d], at_z(-1)).start()

    def column(dy):
        return kv.at[:, (y + dy + NY) % NY, c]

    def half(dy, up):
        return kv.at[pl.ds(0 if up else NZ // 2, NZ // 2), (y + dy + NY) % NY, c]

    partner = z * NYC + y * 2 + 1 - c

    def kv_rows(step):
        if step == 0:
            kv_send(column(0), yu_sem.at[0], at_y(1), 1).start()
            kv_send(column(0), yd_sem.at[0], at_y(-1), 1).start()
            kv_send(column(0), pc_sem.at[0], partner, 2).start()
        elif step == 1:
            kv_send(column(-1), yu_sem.at[0], at_y(1), 1).wait_recv()
            kv_send(half(-1, True), yu_sem.at[1], at_y(1), 1).start()
            kv_send(column(-1), pc_sem.at[1], partner, 2).start()
            kv_send(column(1), yd_sem.at[0], at_y(-1), 1).wait_recv()
            kv_send(half(1, False), yd_sem.at[1], at_y(-1), 1).start()
            kv_send(column(1), pc_sem.at[2], partner, 2).start()
        elif step == 2:
            kv_send(half(2, True), yu_sem.at[1], at_y(1), 1).wait_recv()
            kv_send(half(2, False), yd_sem.at[1], at_y(-1), 1).wait_recv()
            kv_send(column(2), pc_sem.at[3], partner, 2).start()
        else:
            for k, dy in enumerate((0, -1, 1, 2)):
                other = kv.at[:, (y + dy + NY) % NY, 1 - c]
                kv_send(other, pc_sem.at[k], partner, 2).wait_recv()

    def kv_step(d):
        kv_up(d)
        if d < NZ // 2:
            kv_down(d)

    def attend(_):
        lane = lax.broadcasted_iota(jnp.int32, (SEQ, 2 * HEAD), 1)
        q = q_ref[...].astype(F32) * (HEAD**-0.5)
        q = jnp.concatenate([jnp.where(lane < HEAD, q, 0.0), jnp.where(lane < HEAD, 0.0, q)], axis=0).astype(BF)
        own_gate = gate_ref[0:1, pl.ds(pl.multiple_of(me * SEQ, SEQ), SEQ)]
        column_gate = jnp.transpose(jnp.broadcast_to(own_gate, (SEQ, SEQ)))[:, 0:1]
        gq = jnp.concatenate([column_gate, column_gate], axis=0)
        wide = NYC * SEQ

        def scored(plane):
            keys = []
            for k in range(NYC):
                block = kv[plane, k // 2, k % 2, 0:HEAD, :]
                keys.append(jnp.concatenate([block, block], axis=0))
            gk = gate_ref[0:1, pl.ds(pl.multiple_of(plane * wide, wide), wide)]
            return mm(q, jnp.concatenate(keys, axis=1)) + (gq - gk)

        def folded(w):
            total = w[:, 0:SEQ]
            for k in range(1, NYC):
                total = total + w[:, k * SEQ : (k + 1) * SEQ]
            return total

        def mixed(plane, w):
            values = []
            for k in range(NYC):
                block = kv[plane, k // 2, k % 2, HEAD : 2 * HEAD, :]
                values.append(jnp.concatenate([block, block], axis=0))
            return lax.dot_general(
                w.astype(BF), jnp.concatenate(values, axis=1), (((1,), (1,)), ((), ())), preferred_element_type=F32
            )

        rows = lax.broadcasted_iota(jnp.int32, (2 * SEQ, wide), 0) & (SEQ - 1)
        cols = lax.broadcasted_iota(jnp.int32, (2 * SEQ, wide), 1)
        s = jnp.where(cols <= rows + yc * SEQ, scored(z), -jnp.inf)
        best = jnp.max(s, axis=1, keepdims=True)
        w = jnp.exp(s - best)

        def plane_step(plane, state):
            best, total, summed = state
            s = scored(plane)
            new = jnp.maximum(best, jnp.max(s, axis=1, keepdims=True))
            factor = jnp.exp(best - new)
            w = jnp.exp(s - new)
            return new, total * factor + folded(w), summed * factor + mixed(plane, w)

        best, total, summed = lax.fori_loop(0, z, plane_step, (best, folded(w), mixed(z, w)))
        result = summed / jnp.sum(total, axis=1, keepdims=True)
        result = jnp.where(lane < HEAD, result[0:SEQ, :], result[SEQ : 2 * SEQ, :])
        att[...] = result.astype(BF)
        for k, x in enumerate((right, left, opp)):
            att_send(k, x).start()
        att_all[t] = att[pl.ds(pl.multiple_of(t * MIX, MIX), MIX), :]

    def att_send(k, x):
        return pltpu.make_async_remote_copy(
            src_ref=att.at[pl.ds(pl.multiple_of(x * MIX, MIX), MIX), :], dst_ref=att_all.at[t],
            send_sem=ts_sem, recv_sem=t_sem.at[k], device_id=(me, x), device_id_type=MESH,
        )

    def project(_):
        for k, x in enumerate((left, right, opp)):
            pltpu.make_async_remote_copy(
                src_ref=att_all.at[x], dst_ref=att_all.at[x], send_sem=ts_sem, recv_sem=t_sem.at[k],
                device_id=(me, x), device_id_type=MESH,
            ).wait_recv()
        loads[4].wait()
        joined = jnp.concatenate([att_all[k] for k in range(NT)], axis=1)
        mix_ref[...] = mm(joined, wo[...]).astype(BF)

    own = pl.ds(pl.multiple_of(t * ROWS, ROWS), ROWS)
    tokens = NT * ROWS
    r = routes_ref[...]
    r0 = r[0:1, :]
    r1 = r[1:2, :]
    expert = lax.broadcasted_iota(jnp.int32, (NE, tokens), 0)
    s0 = jnp.where(r0 == expert, 1.0, 0.0)
    s1 = jnp.where(r1 == expert, 1.0, 0.0)
    ta = lax.broadcasted_iota(jnp.int32, (tokens, tokens), 0)
    tb = lax.broadcasted_iota(jnp.int32, (tokens, tokens), 1)
    earlier = jnp.where((ta < tb) & ((ta >> 6) == (tb >> 6)), 1.0, 0.0).astype(BF)
    before = mm((s0 + s1).astype(BF), earlier)
    slot0 = r0.astype(F32) * CAP + jnp.sum(before * s0, axis=0, keepdims=True)
    slot1 = r1.astype(F32) * CAP + jnp.sum((before + s0) * s1, axis=0, keepdims=True)

    slot = lax.broadcasted_iota(jnp.int32, (SL, tokens), 0).astype(F32)
    pick[0:tokens, :] = jnp.transpose(jnp.where(slot0 == slot, 1.0, 0.0)).astype(BF)
    pick[tokens : 2 * tokens, :] = jnp.transpose(jnp.where(slot1 == slot, 1.0, 0.0)).astype(BF)
    wcol[...] = jnp.transpose(jnp.concatenate([rw_ref[...], jnp.zeros((6, tokens), F32)], axis=0))
    both = jnp.concatenate([pick[own, :], pick[pl.ds(pl.multiple_of(tokens + t * ROWS, ROWS), ROWS), :]], axis=0)

    loads[0].wait()

    def normalise(rows):
        wide = xin[rows, :].astype(F32)
        scale = lax.rsqrt(jnp.mean(wide * wide, axis=-1, keepdims=True) + 1e-06)
        normed[rows, :] = (wide * scale * gain_ref[...].astype(F32)[None, :]).astype(BF)

    normalise(own)
    chosen = jnp.transpose(both[0:ROWS, :].astype(F32) + both[ROWS : 2 * ROWS, :].astype(F32)).astype(BF)
    obuf[...] = mm(chosen, normed[own, :]).astype(BF)
    for g in range(SL // 16):
        rows_to_tiles(perm, obuf, 16 * g, send, 256 * g)

    loads[5].wait()
    loads[6].wait()
    pl.semaphore_wait(barrier, NE - 1 + 3)

    sendp4 = sendp.reshape(len(FULL) * NT, QR, 128)

    def dispatch(q):
        far = ((z + DZ[q]) % NZ) * NYC

        def ship(j, _):
            place = (yc + j) % NYC
            to = far + place
            if q in FULL:
                src = sendp4.at[
                    pl.ds(FULL.index(q) * NT, NT), pl.ds(pl.multiple_of(place * CH, CH), CH), :
                ]
                dst = recv.at[:, pl.ds(pl.multiple_of(q * QR + yc * CH, CH), CH), :]
            else:
                src = send.at[pl.ds(pl.multiple_of(to * CH, CH), CH), :]
                dst = recv.at[t, pl.ds(pl.multiple_of(q * QR + yc * CH, CH), CH), :]
            pltpu.make_async_remote_copy(
                src_ref=src, dst_ref=dst, send_sem=ap_sem if q in FULL else as_sem, recv_sem=a_sem.at[q],
                device_id=(to, t), device_id_type=MESH,
            ).start()
            return 0

        lax.fori_loop(1 if q == 0 else 0, NYC, ship, 0)

    for q in ISSUE:
        if q not in FULL:
            dispatch(q)
    recv[t, pl.ds(pl.multiple_of(yc * CH, CH), CH), :] = send[pl.ds(pl.multiple_of(me * CH, CH), CH), :]

    for b in range(NT):
        normalise(pl.ds(b * ROWS, ROWS))
    lane = lax.broadcasted_iota(jnp.int32, (BLK, tokens), 1)
    row = lax.broadcasted_iota(jnp.int32, (BLK, tokens), 0).astype(F32)
    named = []
    for q in FULL:
        goal = row + (((z + DZ[q]) % NZ) * BLK).astype(F32)
        hit = (slot0 == goal) | (slot1 == goal)
        named += [jnp.where(hit & ((lane >> 6) == b), 1.0, 0.0) for b in range(NT)]
    obuf[...] = mm(jnp.concatenate(named, axis=0).astype(BF), normed[...]).astype(BF)
    for g in range(SL // 16):
        rows_to_tiles(perm, obuf, 16 * g, sendp, 256 * g)
    for q in ISSUE:
        if q in FULL:
            dispatch(q)

    def chunk(src, q):
        return recv.at[src, pl.ds(q * QR, QR), :]

    def hop(src, q, sem, x):
        return pltpu.make_async_remote_copy(
            src_ref=chunk(src, q), dst_ref=chunk(src, q), send_sem=xs_sem, recv_sem=sem.at[q],
            device_id=(me, x), device_id_type=MESH,
        )

    def arrive(q):
        n = QR - CH if q == 0 else QR
        dst = recv.at[:, pl.ds(q * QR, n), :] if q in FULL else recv.at[t, pl.ds(q * QR, n), :]
        pltpu.make_async_remote_copy(
            src_ref=dst, dst_ref=dst,
            send_sem=as_sem, recv_sem=a_sem.at[q], device_id=(me, right), device_id_type=MESH,
        ).wait_recv()

    def spread(q):
        arrive(q)
        if q in FULL:
            return
        hop(t, q, gl_sem, right).start()
        hop(t, q, gr_sem, left).start()

    def clockwise(q):
        return PARTS.index(q) % 2 == 0

    def relay(q):
        if q in FULL:
            return
        if clockwise(q):
            hop(left, q, gl_sem, right).wait_recv()
            hop(left, q, g2_sem, right).start()
        else:
            hop(right, q, gr_sem, left).wait_recv()
            hop(right, q, g2_sem, left).start()

    def gathered(q):
        if q in FULL:
            return
        if clockwise(q):
            hop(right, q, gr_sem, left).wait_recv()
        else:
            hop(left, q, gl_sem, right).wait_recv()
        hop(opp, q, g2_sem, right).wait_recv()

    def rsend(src, dst, sem, p, x):
        return pltpu.make_async_remote_copy(
            src_ref=src, dst_ref=dst.at[p], send_sem=rr_sem, recv_sem=sem.at[p], device_id=(me, x), device_id_type=MESH
        )

    def ways(p):
        return (right, left) if p % 2 == 0 else (left, right)

    first = next(step for step in ORDER if step[0] == "experts")

    def experts(p):
        gathered(2 * p)
        gathered(2 * p + 1)
        if ("experts", p) == first:
            for load in loads[1:4]:
                load.wait()
        for tt in range(NT):
            for g in range(PT // 16):
                at = p * 2 * QR + g * 256
                y = mm(perm, recv[tt, at : at + 256, :]).astype(BF)
                row = tt * PT + 16 * g
                for i in range(TR):
                    xb[row : row + 16, 128 * i : 128 * i + 128] = y[16 * i : 16 * i + 16, :]
        x = xb[...]
        gate = mm(x, wg[...])
        up = mm(x, wu[...])
        hidden = (gate / (1.0 + jnp.exp(-gate)) * up).astype(BF)
        for tt in range(NT):
            part[p, tt] = mm(hidden[tt * PT : (tt + 1) * PT, :], wd[...]).astype(BF)
        fwd, bwd = ways(p)
        rsend(part.at[p, opp], rs1, r1_sem, p, fwd).start()
        rsend(part.at[p, bwd], rss, rss_sem, p, bwd).start()

    def middle(p):
        fwd, bwd = ways(p)
        rsend(part.at[p, opp], rs1, r1_sem, p, fwd).wait_recv()
        sumb[p] = (rs1[p].astype(F32) + part[p, fwd].astype(F32)).astype(BF)
        rsend(sumb.at[p], rsd, rsd_sem, p, fwd).start()

    def finish(p):
        fwd, bwd = ways(p)
        rsend(part.at[p, bwd], rss, rss_sem, p, bwd).wait_recv()
        rsend(sumb.at[p], rsd, rsd_sem, p, fwd).wait_recv()
        tot[...] = (part[p, t].astype(F32) + rss[p].astype(F32) + rsd[p].astype(F32)).astype(BF)
        for g in range(PT // 16):
            rows_to_tiles(perm, tot, 16 * g, ret, p * 2 * QR + 256 * g)
        for q in (2 * p, 2 * p + 1):
            far = ((z + NZ - DZ[q]) % NZ) * NYC

            def home(j, _, q=q, far=far):
                to = (yc + j) % NYC
                pltpu.make_async_remote_copy(
                    src_ref=ret.at[pl.ds(pl.multiple_of(q * QR + to * CH, CH), CH), :],
                    dst_ref=back.at[pl.ds(pl.multiple_of(me * CH, CH), CH), :],
                    send_sem=bs_sem,
                    recv_sem=b_sem,
                    device_id=(far + to, t),
                    device_id_type=MESH,
                ).start()
                return 0

            lax.fori_loop(1 if q == 0 else 0, NYC, home, 0)
        if p == 0:
            back[pl.ds(pl.multiple_of(me * CH, CH), CH), :] = ret[pl.ds(pl.multiple_of(yc * CH, CH), CH), :]

    steps = dict(
        spread=spread, relay=relay, experts=experts, middle=middle, finish=finish, kv=kv_step, rows=kv_rows,
        attend=attend, project=project,
    )
    for name, index in ORDER:
        steps[name](index)

    n = ALL - CH
    last = pltpu.make_async_remote_copy(
        src_ref=ret.at[pl.ds(0, n), :], dst_ref=back.at[pl.ds(0, n), :], send_sem=bs_sem, recv_sem=b_sem,
        device_id=(me, right), device_id_type=MESH,
    )
    last.wait_recv()
    for g in range(SL // 16):
        y = mm(perm, back[256 * g : 256 * g + 256, :]).astype(BF)
        for i in range(TR):
            resb[16 * g : 16 * g + 16, 128 * i : 128 * i + 128] = y[16 * i : 16 * i + 16, :]
    picked = mm(both, resb[...])
    w = wcol[own, :]
    out_ref[...] = (w[:, 0:1] * picked[0:ROWS, :] + w[:, 1:2] * picked[ROWS : 2 * ROWS, :]).astype(BF)

    last.wait_send()
    pltpu.make_async_remote_copy(
        src_ref=kv.at[:, pl.ds(0, 3), 0], dst_ref=kv.at[:, pl.ds(0, 3), 0], send_sem=ks_sem.at[1], recv_sem=ku_sem.at[0],
        device_id=(me, right), device_id_type=MESH,
    ).wait_send()
    pltpu.make_async_remote_copy(
        src_ref=kv.at[:, :, 0], dst_ref=kv.at[:, :, 0], send_sem=ks_sem.at[2], recv_sem=ku_sem.at[0],
        device_id=(me, right), device_id_type=MESH,
    ).wait_send()
    pltpu.make_async_remote_copy(
        src_ref=kv.at[pl.ds(0, NZ - 1), 0, 0], dst_ref=kv.at[pl.ds(0, NZ - 1), 0, 0], send_sem=ks_sem.at[0],
        recv_sem=ku_sem.at[0], device_id=(me, right), device_id_type=MESH,
    ).wait_send()
    pltpu.make_async_remote_copy(
        src_ref=att.at[pl.ds(0, 3 * MIX), :], dst_ref=att.at[pl.ds(0, 3 * MIX), :], send_sem=ts_sem,
        recv_sem=t_sem.at[0], device_id=(me, right), device_id_type=MESH,
    ).wait_send()
    n = len(PARTS) * QR - CH
    pltpu.make_async_remote_copy(
        src_ref=send.at[pl.ds(0, n), :], dst_ref=send.at[pl.ds(0, n), :], send_sem=as_sem, recv_sem=a_sem.at[0],
        device_id=(me, right), device_id_type=MESH,
    ).wait_send()
    pltpu.make_async_remote_copy(
        src_ref=sendp, dst_ref=sendp, send_sem=ap_sem, recv_sem=a_sem.at[0],
        device_id=(me, right), device_id_type=MESH,
    ).wait_send()
    n = len(PARTS) * QR
    pltpu.make_async_remote_copy(
        src_ref=recv.at[pl.ds(0, 3), pl.ds(0, n), :], dst_ref=recv.at[pl.ds(0, 3), pl.ds(0, n), :], send_sem=xs_sem,
        recv_sem=gl_sem.at[0], device_id=(me, right), device_id_type=MESH,
    ).wait_send()
    pltpu.make_async_remote_copy(
        src_ref=part.at[:, pl.ds(0, 3)], dst_ref=part.at[:, pl.ds(0, 3)], send_sem=rr_sem, recv_sem=r1_sem.at[0],
        device_id=(me, right), device_id_type=MESH,
    ).wait_send()


def body(
    queries,
    key_cache,
    value_cache,
    cum_gate,
    out_weight,
    routed_input,
    norm_gain,
    routes,
    route_weight,
    expert_gate,
    expert_up,
    expert_down,
):
    vmem = pl.BlockSpec(memory_space=pltpu.VMEM)
    hbm = pl.BlockSpec(memory_space=pl.ANY)
    dma = pltpu.SemaphoreType.DMA
    expert_out, mixed_out = pl.pallas_call(
        layer_kernel,
        out_shape=(jax.ShapeDtypeStruct((ROWS, D), BF), jax.ShapeDtypeStruct((MIX, D), BF)),
        in_specs=[hbm, vmem, vmem, vmem, hbm, hbm, hbm, vmem, hbm, hbm, vmem, hbm],
        out_specs=(vmem, vmem),
        scratch_shapes=[
            pltpu.VMEM((NT * ROWS, D), BF),
            pltpu.VMEM((NT * ROWS, D), BF),
            pltpu.VMEM((SL, D), BF),
            pltpu.VMEM((2 * NT * ROWS, SL), BF),
            pltpu.VMEM((NT * ROWS, 8), F32),
            pltpu.VMEM((ALL, 128), BF),
            pltpu.VMEM((len(FULL) * NT * QR, 128), BF),
            pltpu.VMEM((NT, ALL, 128), BF),
            pltpu.VMEM((D, HID), BF),
            pltpu.VMEM((D, HID), BF),
            pltpu.VMEM((HID, D), BF),
            pltpu.VMEM((NT * PT, D), BF),
            pltpu.VMEM((NP, NT, PT, D), BF),
            pltpu.VMEM((NP, PT, D), BF),
            pltpu.VMEM((NP, PT, D), BF),
            pltpu.VMEM((NP, PT, D), BF),
            pltpu.VMEM((NP, PT, D), BF),
            pltpu.VMEM((PT, D), BF),
            pltpu.VMEM((ALL, 128), BF),
            pltpu.VMEM((ALL, 128), BF),
            pltpu.VMEM((SL, D), BF),
            pltpu.VMEM((NZ, NY, 2, 2 * HEAD, SEQ), BF),
            pltpu.VMEM((NT * 2 * HEAD, D), BF),
            pltpu.VMEM((SEQ, 2 * HEAD), BF),
            pltpu.VMEM((NT, MIX, 2 * HEAD), BF),
            dma((7,)),
            dma,
            dma,
            dma((NZ,)),
            dma,
            dma((NZ,)),
            dma((NZ,)),
            dma((NZ,)),
            dma,
            dma((NP,)),
            dma((NP,)),
            dma((NP,)),
            dma,
            dma,
            dma((3,)),
            dma((4,)),
            dma((3,)),
            dma((2,)),
            dma((2,)),
            dma((4,)),
            dma,
            dma((3,)),
        ],
        compiler_params=pltpu.CompilerParams(collective_id=0, has_side_effects=True, vmem_limit_bytes=67043328),
        cost_estimate=pl.CostEstimate(flops=60_000_000_000, bytes_accessed=8_000_000, transcendentals=0),
        name="layer",
    )(
        routed_input, routes.T, route_weight.T, norm_gain,
        expert_gate[0], expert_up[0], expert_down[0],
        queries, key_cache[0], value_cache[0], cum_gate, out_weight,
    )
    return (mixed_out, expert_out)


def solution(mesh):
    return jax.shard_map(
        body,
        mesh=mesh,
        in_specs=(
            P("ep", "tp"),
            P("tp", None, "ep"),
            P("tp", None, "ep"),
            P("tp", None),
            P(),
            P("ep", None),
            P(),
            P("ep", None),
            P("ep", None),
            P("ep", None, "tp"),
            P("ep", None, "tp"),
            P("ep", "tp", None),
        ),
        out_specs=(P(("ep", "tp"), None), P(("ep", "tp"), None)),
        check_vma=False,
    )
```

```python
import jax
import jax.numpy as jnp
from jax import lax
from jax.experimental import pallas as pl
from jax.experimental.pallas import tpu as pltpu
from jax.sharding import PartitionSpec as P

MESH = pl.DeviceIdType.MESH
BF = jnp.bfloat16
F32 = jnp.float32

D = 2048
ROWS = 64
CAP = 3
NT = 4
NZ = 8
NYC = 8
NE = NZ * NYC
SL = NE * CAP
TR = D // 128
CH = CAP * TR
QR = NYC * CH
ALL = NE * CH
NP = NZ // 2
PT = 2 * NYC * CAP
HID = 256
NY = 4
HEAD = 64
SEQ = 128
MIX = SEQ // NT
DZ = (0, 1, 7, 2, 3, 6, 5, 4)
ISSUE = (4, 5, 0, 6, 3, 7, 2, 1)
FULL = tuple(q for q in range(NZ) if DZ[q] in (1, 7))
PARTS = tuple(q for q in range(NZ) if q not in FULL)
BLK = NYC * CAP
ORDER = (
    ("spread", 0), ("spread", 5), ("spread", 4), ("relay", 0), ("relay", 5), ("spread", 3),
    ("spread", 6), ("relay", 4), ("spread", 7), ("relay", 6), ("relay", 3), ("relay", 7),
    ("kv", 0), ("experts", 2), ("spread", 2), ("spread", 1), ("kv", 1), ("experts", 3),
    ("kv", 2), ("kv", 3), ("middle", 2), ("experts", 1), ("kv", 4), ("rows", 0),
    ("middle", 3), ("finish", 2), ("middle", 1), ("experts", 0), ("rows", 1), ("finish", 3),
    ("middle", 0), ("rows", 2), ("finish", 1), ("rows", 3), ("finish", 0), ("attend", 0),
    ("project", 0),
)


def permutation():
    a = lax.broadcasted_iota(jnp.int32, (256, 256), 0)
    b = lax.broadcasted_iota(jnp.int32, (256, 256), 1)
    hit = ((a & 15) == (b >> 4)) & ((a >> 4) == (b & 15))
    return hit.astype(F32).astype(BF)


def mm(a, b):
    return jnp.dot(a, b, preferred_element_type=F32)


def rows_to_tiles(perm, src, row, dst, at):
    z = jnp.concatenate([src[row : row + 16, 128 * i : 128 * i + 128] for i in range(TR)], axis=0)
    dst[at : at + 256, :] = mm(perm, z).astype(BF)


def layer_kernel(
    x_ref, routes_ref, rw_ref, gain_ref, wg_hbm, wu_hbm, wd_hbm, q_ref, key_hbm, value_hbm, gate_ref, wo_hbm,
    out_ref, mix_ref,
    xin, normed, obuf, pick, wcol, send, sendp, recv, wg, wu, wd, xb, part, rs1, rss, rsd, sumb, tot, ret, back, resb, kv, wo, att, att_all,
    ld_sem, as_sem, ap_sem, a_sem, xs_sem, gl_sem, gr_sem, g2_sem, rr_sem, r1_sem, rss_sem, rsd_sem, bs_sem, b_sem,
    ks_sem, ku_sem, kd_sem, yu_sem, yd_sem, pc_sem, ts_sem, t_sem,
):
    t = lax.axis_index("tp")
    me = lax.axis_index("ep")
    z = me // NYC
    yc = me % NYC
    y = yc // 2
    c = yc % 2
    right = (t + 1) % NT
    left = (t + 3) % NT
    opp = (t + 2) % NT

    loads = [
        pltpu.make_async_copy(x_ref, xin, ld_sem.at[0]),
        pltpu.make_async_copy(wg_hbm, wg, ld_sem.at[1]),
        pltpu.make_async_copy(wu_hbm, wu, ld_sem.at[2]),
        pltpu.make_async_copy(wd_hbm, wd, ld_sem.at[3]),
        pltpu.make_async_copy(wo_hbm, wo, ld_sem.at[4]),
        pltpu.make_async_copy(key_hbm, kv.at[z, y, c, pl.ds(0, HEAD), :], ld_sem.at[5]),
        pltpu.make_async_copy(value_hbm, kv.at[z, y, c, pl.ds(HEAD, HEAD), :], ld_sem.at[6]),
    ]
    for load in loads:
        load.start()

    barrier = pltpu.get_barrier_semaphore()

    def greet(k, _):
        pl.semaphore_signal(barrier, inc=1, device_id=((me + k) % NE, t), device_id_type=MESH)
        return 0

    lax.fori_loop(1, NE, greet, 0)
    for x in (right, left, opp):
        pl.semaphore_signal(barrier, inc=1, device_id=(me, x), device_id_type=MESH)

    perm = permutation()

    def kv_send(block, sem, to, way=0):
        return pltpu.make_async_remote_copy(
            src_ref=block, dst_ref=block, send_sem=ks_sem.at[way], recv_sem=sem, device_id=(to, t), device_id_type=MESH
        )

    def at_z(dz):
        return ((z + dz + NZ) % NZ) * NYC + yc

    def at_y(dy):
        return z * NYC + ((y + dy + NY) % NY) * 2 + c

    def kv_up(d):
        block = kv.at[(z + NZ - d) % NZ, y, c]
        if d > 0:
            kv_send(block, ku_sem.at[d - 1], at_z(1)).wait_recv()
        if d < NZ // 2:
            kv_send(block, ku_sem.at[d], at_z(1)).start()

    def kv_down(d):
        block = kv.at[(z + d) % NZ, y, c]
        if d > 0:
            kv_send(block, kd_sem.at[d - 1], at_z(-1)).wait_recv()
        if d < NZ // 2 - 1:
            kv_send(block, kd_sem.at[d], at_z(-1)).start()

    def column(dy):
        return kv.at[:, (y + dy + NY) % NY, c]

    def half(dy, up):
        return kv.at[pl.ds(0 if up else NZ // 2, NZ // 2), (y + dy + NY) % NY, c]

    partner = z * NYC + y * 2 + 1 - c

    def kv_rows(step):
        if step == 0:
            kv_send(column(0), yu_sem.at[0], at_y(1), 1).start()
            kv_send(column(0), yd_sem.at[0], at_y(-1), 1).start()
            kv_send(column(0), pc_sem.at[0], partner, 2).start()
        elif step == 1:
            kv_send(column(-1), yu_sem.at[0], at_y(1), 1).wait_recv()
            kv_send(half(-1, True), yu_sem.at[1], at_y(1), 1).start()
            kv_send(column(-1), pc_sem.at[1], partner, 2).start()
            kv_send(column(1), yd_sem.at[0], at_y(-1), 1).wait_recv()
            kv_send(half(1, False), yd_sem.at[1], at_y(-1), 1).start()
            kv_send(column(1), pc_sem.at[2], partner, 2).start()
        elif step == 2:
            kv_send(half(2, True), yu_sem.at[1], at_y(1), 1).wait_recv()
            kv_send(half(2, False), yd_sem.at[1], at_y(-1), 1).wait_recv()
            kv_send(column(2), pc_sem.at[3], partner, 2).start()
        else:
            for k, dy in enumerate((0, -1, 1, 2)):
                other = kv.at[:, (y + dy + NY) % NY, 1 - c]
                kv_send(other, pc_sem.at[k], partner, 2).wait_recv()

    def kv_step(d):
        kv_up(d)
        if d < NZ // 2:
            kv_down(d)

    def attend(_):
        lane = lax.broadcasted_iota(jnp.int32, (SEQ, 2 * HEAD), 1)
        q = q_ref[...].astype(F32) * (HEAD**-0.5)
        q = jnp.concatenate([jnp.where(lane < HEAD, q, 0.0), jnp.where(lane < HEAD, 0.0, q)], axis=0).astype(BF)
        own_gate = gate_ref[0:1, pl.ds(pl.multiple_of(me * SEQ, SEQ), SEQ)]
        column_gate = jnp.transpose(jnp.broadcast_to(own_gate, (SEQ, SEQ)))[:, 0:1]
        gq = jnp.concatenate([column_gate, column_gate], axis=0)
        wide = NYC * SEQ

        def scored(plane):
            keys = []
            for k in range(NYC):
                block = kv[plane, k // 2, k % 2, 0:HEAD, :]
                keys.append(jnp.concatenate([block, block], axis=0))
            gk = gate_ref[0:1, pl.ds(pl.multiple_of(plane * wide, wide), wide)]
            return mm(q, jnp.concatenate(keys, axis=1)) + (gq - gk)

        def folded(w):
            total = w[:, 0:SEQ]
            for k in range(1, NYC):
                total = total + w[:, k * SEQ : (k + 1) * SEQ]
            return total

        def mixed(plane, w):
            values = []
            for k in range(NYC):
                block = kv[plane, k // 2, k % 2, HEAD : 2 * HEAD, :]
                values.append(jnp.concatenate([block, block], axis=0))
            return lax.dot_general(
                w.astype(BF), jnp.concatenate(values, axis=1), (((1,), (1,)), ((), ())), preferred_element_type=F32
            )

        rows = lax.broadcasted_iota(jnp.int32, (2 * SEQ, wide), 0) & (SEQ - 1)
        cols = lax.broadcasted_iota(jnp.int32, (2 * SEQ, wide), 1)
        s = jnp.where(cols <= rows + yc * SEQ, scored(z), -jnp.inf)
        best = jnp.max(s, axis=1, keepdims=True)
        w = jnp.exp(s - best)

        def plane_step(plane, state):
            best, total, summed = state
            s = scored(plane)
            new = jnp.maximum(best, jnp.max(s, axis=1, keepdims=True))
            factor = jnp.exp(best - new)
            w = jnp.exp(s - new)
            return new, total * factor + folded(w), summed * factor + mixed(plane, w)

        best, total, summed = lax.fori_loop(0, z, plane_step, (best, folded(w), mixed(z, w)))
        result = summed / jnp.sum(total, axis=1, keepdims=True)
        result = jnp.where(lane < HEAD, result[0:SEQ, :], result[SEQ : 2 * SEQ, :])
        att[...] = result.astype(BF)
        for k, x in enumerate((right, left, opp)):
            att_send(k, x).start()
        att_all[t] = att[pl.ds(pl.multiple_of(t * MIX, MIX), MIX), :]

    def att_send(k, x):
        return pltpu.make_async_remote_copy(
            src_ref=att.at[pl.ds(pl.multiple_of(x * MIX, MIX), MIX), :], dst_ref=att_all.at[t],
            send_sem=ts_sem, recv_sem=t_sem.at[k], device_id=(me, x), device_id_type=MESH,
        )

    def project(_):
        for k, x in enumerate((left, right, opp)):
            pltpu.make_async_remote_copy(
                src_ref=att_all.at[x], dst_ref=att_all.at[x], send_sem=ts_sem, recv_sem=t_sem.at[k],
                device_id=(me, x), device_id_type=MESH,
            ).wait_recv()
        loads[4].wait()
        joined = jnp.concatenate([att_all[k] for k in range(NT)], axis=1)
        mix_ref[...] = mm(joined, wo[...]).astype(BF)

    own = pl.ds(pl.multiple_of(t * ROWS, ROWS), ROWS)
    tokens = NT * ROWS
    r = routes_ref[...]
    r0 = r[0:1, :]
    r1 = r[1:2, :]
    expert = lax.broadcasted_iota(jnp.int32, (NE, tokens), 0)
    s0 = jnp.where(r0 == expert, 1.0, 0.0)
    s1 = jnp.where(r1 == expert, 1.0, 0.0)
    ta = lax.broadcasted_iota(jnp.int32, (tokens, tokens), 0)
    tb = lax.broadcasted_iota(jnp.int32, (tokens, tokens), 1)
    earlier = jnp.where((ta < tb) & ((ta >> 6) == (tb >> 6)), 1.0, 0.0).astype(BF)
    before = mm((s0 + s1).astype(BF), earlier)
    slot0 = r0.astype(F32) * CAP + jnp.sum(before * s0, axis=0, keepdims=True)
    slot1 = r1.astype(F32) * CAP + jnp.sum((before + s0) * s1, axis=0, keepdims=True)

    slot = lax.broadcasted_iota(jnp.int32, (SL, tokens), 0).astype(F32)
    pick[0:tokens, :] = jnp.transpose(jnp.where(slot0 == slot, 1.0, 0.0)).astype(BF)
    pick[tokens : 2 * tokens, :] = jnp.transpose(jnp.where(slot1 == slot, 1.0, 0.0)).astype(BF)
    wcol[...] = jnp.transpose(jnp.concatenate([rw_ref[...], jnp.zeros((6, tokens), F32)], axis=0))
    both = jnp.concatenate([pick[own, :], pick[pl.ds(pl.multiple_of(tokens + t * ROWS, ROWS), ROWS), :]], axis=0)

    loads[0].wait()

    def normalise(rows):
        wide = xin[rows, :].astype(F32)
        scale = lax.rsqrt(jnp.mean(wide * wide, axis=-1, keepdims=True) + 1e-06)
        normed[rows, :] = (wide * scale * gain_ref[...].astype(F32)[None, :]).astype(BF)

    normalise(own)
    chosen = jnp.transpose(both[0:ROWS, :].astype(F32) + both[ROWS : 2 * ROWS, :].astype(F32)).astype(BF)
    obuf[...] = mm(chosen, normed[own, :]).astype(BF)
    for g in range(SL // 16):
        rows_to_tiles(perm, obuf, 16 * g, send, 256 * g)

    loads[5].wait()
    loads[6].wait()
    pl.semaphore_wait(barrier, NE - 1 + 3)

    sendp4 = sendp.reshape(len(FULL) * NT, QR, 128)

    def dispatch(q):
        far = ((z + DZ[q]) % NZ) * NYC

        def ship(j, _):
            place = (yc + j) % NYC
            to = far + place
            if q in FULL:
                src = sendp4.at[
                    pl.ds(FULL.index(q) * NT, NT), pl.ds(pl.multiple_of(place * CH, CH), CH), :
                ]
                dst = recv.at[:, pl.ds(pl.multiple_of(q * QR + yc * CH, CH), CH), :]
            else:
                src = send.at[pl.ds(pl.multiple_of(to * CH, CH), CH), :]
                dst = recv.at[t, pl.ds(pl.multiple_of(q * QR + yc * CH, CH), CH), :]
            pltpu.make_async_remote_copy(
                src_ref=src, dst_ref=dst, send_sem=ap_sem if q in FULL else as_sem, recv_sem=a_sem.at[q],
                device_id=(to, t), device_id_type=MESH,
            ).start()
            return 0

        lax.fori_loop(1 if q == 0 else 0, NYC, ship, 0)

    for q in ISSUE:
        if q not in FULL:
            dispatch(q)
    recv[t, pl.ds(pl.multiple_of(yc * CH, CH), CH), :] = send[pl.ds(pl.multiple_of(me * CH, CH), CH), :]

    for b in range(NT):
        normalise(pl.ds(b * ROWS, ROWS))
    lane = lax.broadcasted_iota(jnp.int32, (BLK, tokens), 1)
    row = lax.broadcasted_iota(jnp.int32, (BLK, tokens), 0).astype(F32)
    named = []
    for q in FULL:
        goal = row + (((z + DZ[q]) % NZ) * BLK).astype(F32)
        hit = (slot0 == goal) | (slot1 == goal)
        named += [jnp.where(hit & ((lane >> 6) == b), 1.0, 0.0) for b in range(NT)]
    obuf[...] = mm(jnp.concatenate(named, axis=0).astype(BF), normed[...]).astype(BF)
    for g in range(SL // 16):
        rows_to_tiles(perm, obuf, 16 * g, sendp, 256 * g)
    for q in ISSUE:
        if q in FULL:
            dispatch(q)

    def chunk(src, q):
        return recv.at[src, pl.ds(q * QR, QR), :]

    def hop(src, q, sem, x):
        return pltpu.make_async_remote_copy(
            src_ref=chunk(src, q), dst_ref=chunk(src, q), send_sem=xs_sem, recv_sem=sem.at[q],
            device_id=(me, x), device_id_type=MESH,
        )

    def arrive(q):
        n = QR - CH if q == 0 else QR
        dst = recv.at[:, pl.ds(q * QR, n), :] if q in FULL else recv.at[t, pl.ds(q * QR, n), :]
        pltpu.make_async_remote_copy(
            src_ref=dst, dst_ref=dst,
            send_sem=as_sem, recv_sem=a_sem.at[q], device_id=(me, right), device_id_type=MESH,
        ).wait_recv()

    def spread(q):
        arrive(q)
        if q in FULL:
            return
        hop(t, q, gl_sem, right).start()
        hop(t, q, gr_sem, left).start()

    def clockwise(q):
        return PARTS.index(q) % 2 == 0

    def relay(q):
        if q in FULL:
            return
        if clockwise(q):
            hop(left, q, gl_sem, right).wait_recv()
            hop(left, q, g2_sem, right).start()
        else:
            hop(right, q, gr_sem, left).wait_recv()
            hop(right, q, g2_sem, left).start()

    def gathered(q):
        if q in FULL:
            return
        if clockwise(q):
            hop(right, q, gr_sem, left).wait_recv()
        else:
            hop(left, q, gl_sem, right).wait_recv()
        hop(opp, q, g2_sem, right).wait_recv()

    def rsend(src, dst, sem, p, x):
        return pltpu.make_async_remote_copy(
            src_ref=src, dst_ref=dst.at[p], send_sem=rr_sem, recv_sem=sem.at[p], device_id=(me, x), device_id_type=MESH
        )

    def ways(p):
        return (right, left) if p % 2 == 0 else (left, right)

    first = next(step for step in ORDER if step[0] == "experts")

    def experts(p):
        gathered(2 * p)
        gathered(2 * p + 1)
        if ("experts", p) == first:
            for load in loads[1:4]:
                load.wait()
        for tt in range(NT):
            for g in range(PT // 16):
                at = p * 2 * QR + g * 256
                y = mm(perm, recv[tt, at : at + 256, :]).astype(BF)
                row = tt * PT + 16 * g
                for i in range(TR):
                    xb[row : row + 16, 128 * i : 128 * i + 128] = y[16 * i : 16 * i + 16, :]
        x = xb[...]
        gate = mm(x, wg[...])
        up = mm(x, wu[...])
        hidden = (gate / (1.0 + jnp.exp(-gate)) * up).astype(BF)
        for tt in range(NT):
            part[p, tt] = mm(hidden[tt * PT : (tt + 1) * PT, :], wd[...]).astype(BF)
        fwd, bwd = ways(p)
        rsend(part.at[p, opp], rs1, r1_sem, p, fwd).start()
        rsend(part.at[p, bwd], rss, rss_sem, p, bwd).start()

    def middle(p):
        fwd, bwd = ways(p)
        rsend(part.at[p, opp], rs1, r1_sem, p, fwd).wait_recv()
        sumb[p] = (rs1[p].astype(F32) + part[p, fwd].astype(F32)).astype(BF)
        rsend(sumb.at[p], rsd, rsd_sem, p, fwd).start()

    def finish(p):
        fwd, bwd = ways(p)
        rsend(part.at[p, bwd], rss, rss_sem, p, bwd).wait_recv()
        rsend(sumb.at[p], rsd, rsd_sem, p, fwd).wait_recv()
        tot[...] = (part[p, t].astype(F32) + rss[p].astype(F32) + rsd[p].astype(F32)).astype(BF)
        for g in range(PT // 16):
            rows_to_tiles(perm, tot, 16 * g, ret, p * 2 * QR + 256 * g)
        for q in (2 * p, 2 * p + 1):
            far = ((z + NZ - DZ[q]) % NZ) * NYC

            def home(j, _, q=q, far=far):
                to = (yc + j) % NYC
                pltpu.make_async_remote_copy(
                    src_ref=ret.at[pl.ds(pl.multiple_of(q * QR + to * CH, CH), CH), :],
                    dst_ref=back.at[pl.ds(pl.multiple_of(me * CH, CH), CH), :],
                    send_sem=bs_sem,
                    recv_sem=b_sem,
                    device_id=(far + to, t),
                    device_id_type=MESH,
                ).start()
                return 0

            lax.fori_loop(1 if q == 0 else 0, NYC, home, 0)
        if p == 0:
            back[pl.ds(pl.multiple_of(me * CH, CH), CH), :] = ret[pl.ds(pl.multiple_of(yc * CH, CH), CH), :]

    steps = dict(
        spread=spread, relay=relay, experts=experts, middle=middle, finish=finish, kv=kv_step, rows=kv_rows,
        attend=attend, project=project,
    )
    for name, index in ORDER:
        steps[name](index)

    n = ALL - CH
    last = pltpu.make_async_remote_copy(
        src_ref=ret.at[pl.ds(0, n), :], dst_ref=back.at[pl.ds(0, n), :], send_sem=bs_sem, recv_sem=b_sem,
        device_id=(me, right), device_id_type=MESH,
    )
    last.wait_recv()
    for g in range(SL // 16):
        y = mm(perm, back[256 * g : 256 * g + 256, :]).astype(BF)
        for i in range(TR):
            resb[16 * g : 16 * g + 16, 128 * i : 128 * i + 128] = y[16 * i : 16 * i + 16, :]
    picked = mm(both, resb[...])
    w = wcol[own, :]
    out_ref[...] = (w[:, 0:1] * picked[0:ROWS, :] + w[:, 1:2] * picked[ROWS : 2 * ROWS, :]).astype(BF)

    last.wait_send()
    pltpu.make_async_remote_copy(
        src_ref=kv.at[:, pl.ds(0, 3), 0], dst_ref=kv.at[:, pl.ds(0, 3), 0], send_sem=ks_sem.at[1], recv_sem=ku_sem.at[0],
        device_id=(me, right), device_id_type=MESH,
    ).wait_send()
    pltpu.make_async_remote_copy(
        src_ref=kv.at[:, :, 0], dst_ref=kv.at[:, :, 0], send_sem=ks_sem.at[2], recv_sem=ku_sem.at[0],
        device_id=(me, right), device_id_type=MESH,
    ).wait_send()
    pltpu.make_async_remote_copy(
        src_ref=kv.at[pl.ds(0, NZ - 1), 0, 0], dst_ref=kv.at[pl.ds(0, NZ - 1), 0, 0], send_sem=ks_sem.at[0],
        recv_sem=ku_sem.at[0], device_id=(me, right), device_id_type=MESH,
    ).wait_send()
    pltpu.make_async_remote_copy(
        src_ref=att.at[pl.ds(0, 3 * MIX), :], dst_ref=att.at[pl.ds(0, 3 * MIX), :], send_sem=ts_sem,
        recv_sem=t_sem.at[0], device_id=(me, right), device_id_type=MESH,
    ).wait_send()
    n = len(PARTS) * QR - CH
    pltpu.make_async_remote_copy(
        src_ref=send.at[pl.ds(0, n), :], dst_ref=send.at[pl.ds(0, n), :], send_sem=as_sem, recv_sem=a_sem.at[0],
        device_id=(me, right), device_id_type=MESH,
    ).wait_send()
    pltpu.make_async_remote_copy(
        src_ref=sendp, dst_ref=sendp, send_sem=ap_sem, recv_sem=a_sem.at[0],
        device_id=(me, right), device_id_type=MESH,
    ).wait_send()
    n = len(PARTS) * QR
    pltpu.make_async_remote_copy(
        src_ref=recv.at[pl.ds(0, 3), pl.ds(0, n), :], dst_ref=recv.at[pl.ds(0, 3), pl.ds(0, n), :], send_sem=xs_sem,
        recv_sem=gl_sem.at[0], device_id=(me, right), device_id_type=MESH,
    ).wait_send()
    pltpu.make_async_remote_copy(
        src_ref=part.at[:, pl.ds(0, 3)], dst_ref=part.at[:, pl.ds(0, 3)], send_sem=rr_sem, recv_sem=r1_sem.at[0],
        device_id=(me, right), device_id_type=MESH,
    ).wait_send()


def hand_over(out_ref, mix_ref, out, mix, sems):
    copies = (pltpu.make_async_copy(out_ref, out, sems.at[0]), pltpu.make_async_copy(mix_ref, mix, sems.at[1]))
    for copy in copies:
        copy.start()
    for copy in copies:
        copy.wait()


def body(
    queries,
    key_cache,
    value_cache,
    cum_gate,
    out_weight,
    routed_input,
    norm_gain,
    routes,
    route_weight,
    expert_gate,
    expert_up,
    expert_down,
):
    vmem = pl.BlockSpec(memory_space=pltpu.VMEM)
    hbm = pl.BlockSpec(memory_space=pl.ANY)
    dma = pltpu.SemaphoreType.DMA
    expert_out, mixed_out = pl.pallas_call(
        layer_kernel,
        out_shape=(jax.ShapeDtypeStruct((ROWS, D), BF), jax.ShapeDtypeStruct((MIX, D), BF)),
        in_specs=[hbm, vmem, vmem, vmem, hbm, hbm, hbm, vmem, hbm, hbm, vmem, hbm],
        out_specs=(vmem, vmem),
        scratch_shapes=[
            pltpu.VMEM((NT * ROWS, D), BF),
            pltpu.VMEM((NT * ROWS, D), BF),
            pltpu.VMEM((SL, D), BF),
            pltpu.VMEM((2 * NT * ROWS, SL), BF),
            pltpu.VMEM((NT * ROWS, 8), F32),
            pltpu.VMEM((ALL, 128), BF),
            pltpu.VMEM((len(FULL) * NT * QR, 128), BF),
            pltpu.VMEM((NT, ALL, 128), BF),
            pltpu.VMEM((D, HID), BF),
            pltpu.VMEM((D, HID), BF),
            pltpu.VMEM((HID, D), BF),
            pltpu.VMEM((NT * PT, D), BF),
            pltpu.VMEM((NP, NT, PT, D), BF),
            pltpu.VMEM((NP, PT, D), BF),
            pltpu.VMEM((NP, PT, D), BF),
            pltpu.VMEM((NP, PT, D), BF),
            pltpu.VMEM((NP, PT, D), BF),
            pltpu.VMEM((PT, D), BF),
            pltpu.VMEM((ALL, 128), BF),
            pltpu.VMEM((ALL, 128), BF),
            pltpu.VMEM((SL, D), BF),
            pltpu.VMEM((NZ, NY, 2, 2 * HEAD, SEQ), BF),
            pltpu.VMEM((NT * 2 * HEAD, D), BF),
            pltpu.VMEM((SEQ, 2 * HEAD), BF),
            pltpu.VMEM((NT, MIX, 2 * HEAD), BF),
            dma((7,)),
            dma,
            dma,
            dma((NZ,)),
            dma,
            dma((NZ,)),
            dma((NZ,)),
            dma((NZ,)),
            dma,
            dma((NP,)),
            dma((NP,)),
            dma((NP,)),
            dma,
            dma,
            dma((3,)),
            dma((4,)),
            dma((3,)),
            dma((2,)),
            dma((2,)),
            dma((4,)),
            dma,
            dma((3,)),
        ],
        compiler_params=pltpu.CompilerParams(collective_id=0, has_side_effects=True, vmem_limit_bytes=67043328),
        cost_estimate=pl.CostEstimate(flops=60_000_000_000, bytes_accessed=8_000_000, transcendentals=0),
        name="layer",
    )(
        routed_input, routes.T, route_weight.T, norm_gain,
        expert_gate[0], expert_up[0], expert_down[0],
        queries, key_cache[0], value_cache[0], cum_gate, out_weight,
    )
    expert_out, mixed_out = pl.pallas_call(
        hand_over,
        out_shape=(jax.ShapeDtypeStruct((ROWS, D), BF), jax.ShapeDtypeStruct((MIX, D), BF)),
        in_specs=[vmem] * 2,
        out_specs=(hbm, hbm),
        scratch_shapes=[dma((2,))],
        compiler_params=pltpu.CompilerParams(vmem_limit_bytes=67043328),
        name="hand_over",
    )(expert_out, mixed_out)
    return (mixed_out, expert_out)


def solution(mesh):
    return jax.shard_map(
        body,
        mesh=mesh,
        in_specs=(
            P("ep", "tp"),
            P("tp", None, "ep"),
            P("tp", None, "ep"),
            P("tp", None),
            P(),
            P("ep", None),
            P(),
            P("ep", None),
            P("ep", None),
            P("ep", None, "tp"),
            P("ep", None, "tp"),
            P("ep", "tp", None),
        ),
        out_specs=(P(("ep", "tp"), None), P(("ep", "tp"), None)),
        check_vma=False,
    )
```

```python
import jax
import jax.numpy as jnp
from jax import lax
from jax.experimental import pallas as pl
from jax.experimental.pallas import tpu as pltpu
from jax.sharding import PartitionSpec as P

MESH = pl.DeviceIdType.MESH
BF = jnp.bfloat16
F32 = jnp.float32

D = 2048
ROWS = 64
CAP = 3
NT = 4
NZ = 8
NYC = 8
NE = NZ * NYC
SL = NE * CAP
TR = D // 128
CH = CAP * TR
QR = NYC * CH
ALL = NE * CH
NP = NZ // 2
PT = 2 * NYC * CAP
HID = 256
NY = 4
HEAD = 64
SEQ = 128
MIX = SEQ // NT
DZ = (0, 1, 7, 2, 3, 6, 5, 4)
ISSUE = (4, 5, 0, 6, 3, 7, 2, 1)
FULL = tuple(q for q in range(NZ) if DZ[q] in (1, 7))
PARTS = tuple(q for q in range(NZ) if q not in FULL)
BLK = NYC * CAP
ORDER = (
    ("spread", 0), ("spread", 5), ("spread", 4), ("relay", 0), ("relay", 5), ("spread", 3),
    ("spread", 6), ("relay", 4), ("spread", 7), ("relay", 6), ("relay", 3), ("relay", 7),
    ("kv", 0), ("experts", 2), ("spread", 2), ("spread", 1), ("kv", 1), ("experts", 3),
    ("kv", 2), ("kv", 3), ("middle", 2), ("experts", 1), ("kv", 4), ("rows", 0),
    ("middle", 3), ("finish", 2), ("middle", 1), ("experts", 0), ("rows", 1), ("finish", 3),
    ("middle", 0), ("rows", 2), ("finish", 1), ("rows", 3), ("finish", 0), ("attend", 0),
    ("project", 0),
)


def permutation():
    a = lax.broadcasted_iota(jnp.int32, (256, 256), 0)
    b = lax.broadcasted_iota(jnp.int32, (256, 256), 1)
    hit = ((a & 15) == (b >> 4)) & ((a >> 4) == (b & 15))
    return hit.astype(F32).astype(BF)


def mm(a, b):
    return jnp.dot(a, b, preferred_element_type=F32)


def rows_to_tiles(perm, src, row, dst, at):
    z = jnp.concatenate([src[row : row + 16, 128 * i : 128 * i + 128] for i in range(TR)], axis=0)
    dst[at : at + 256, :] = mm(perm, z).astype(BF)


def layer_kernel(
    x_ref, routes_ref, rw_ref, gain_ref, wg_hbm, wu_hbm, wd_hbm, q_ref, key_hbm, value_hbm, gate_ref, wo_hbm,
    out_ref, mix_ref,
    xin, normed, obuf, pick, wcol, send, sendp, recv, wg, wu, wd, xb, part, rs1, rss, rsd, sumb, tot, ret, back, resb, kv, wo, att, att_all,
    ld_sem, as_sem, ap_sem, a_sem, xs_sem, gl_sem, gr_sem, g2_sem, rr_sem, r1_sem, rss_sem, rsd_sem, bs_sem, b_sem,
    ks_sem, ku_sem, kd_sem, yu_sem, yd_sem, pc_sem, ts_sem, t_sem,
):
    t = lax.axis_index("tp")
    me = lax.axis_index("ep")
    z = me // NYC
    yc = me % NYC
    y = yc // 2
    c = yc % 2
    right = (t + 1) % NT
    left = (t + 3) % NT
    opp = (t + 2) % NT

    loads = [
        pltpu.make_async_copy(x_ref, xin, ld_sem.at[0]),
        pltpu.make_async_copy(wg_hbm, wg, ld_sem.at[1]),
        pltpu.make_async_copy(wu_hbm, wu, ld_sem.at[2]),
        pltpu.make_async_copy(wd_hbm, wd, ld_sem.at[3]),
        pltpu.make_async_copy(wo_hbm, wo, ld_sem.at[4]),
        pltpu.make_async_copy(key_hbm, kv.at[z, y, c, pl.ds(0, HEAD), :], ld_sem.at[5]),
        pltpu.make_async_copy(value_hbm, kv.at[z, y, c, pl.ds(HEAD, HEAD), :], ld_sem.at[6]),
    ]
    for load in loads:
        load.start()

    barrier = pltpu.get_barrier_semaphore()

    def greet(k, _):
        pl.semaphore_signal(barrier, inc=1, device_id=((me + k) % NE, t), device_id_type=MESH)
        return 0

    lax.fori_loop(1, NE, greet, 0)
    for x in (right, left, opp):
        pl.semaphore_signal(barrier, inc=1, device_id=(me, x), device_id_type=MESH)

    perm = permutation()

    def kv_send(block, sem, to, way=0):
        return pltpu.make_async_remote_copy(
            src_ref=block, dst_ref=block, send_sem=ks_sem.at[way], recv_sem=sem, device_id=(to, t), device_id_type=MESH
        )

    def at_z(dz):
        return ((z + dz + NZ) % NZ) * NYC + yc

    def at_y(dy):
        return z * NYC + ((y + dy + NY) % NY) * 2 + c

    def kv_up(d):
        block = kv.at[(z + NZ - d) % NZ, y, c]
        if d > 0:
            kv_send(block, ku_sem.at[d - 1], at_z(1)).wait_recv()
        if d < NZ // 2:
            kv_send(block, ku_sem.at[d], at_z(1)).start()

    def kv_down(d):
        block = kv.at[(z + d) % NZ, y, c]
        if d > 0:
            kv_send(block, kd_sem.at[d - 1], at_z(-1)).wait_recv()
        if d < NZ // 2 - 1:
            kv_send(block, kd_sem.at[d], at_z(-1)).start()

    def column(dy):
        return kv.at[:, (y + dy + NY) % NY, c]

    def half(dy, up):
        return kv.at[pl.ds(0 if up else NZ // 2, NZ // 2), (y + dy + NY) % NY, c]

    partner = z * NYC + y * 2 + 1 - c

    def kv_rows(step):
        if step == 0:
            kv_send(column(0), yu_sem.at[0], at_y(1), 1).start()
            kv_send(column(0), yd_sem.at[0], at_y(-1), 1).start()
            kv_send(column(0), pc_sem.at[0], partner, 2).start()
        elif step == 1:
            kv_send(column(-1), yu_sem.at[0], at_y(1), 1).wait_recv()
            kv_send(half(-1, True), yu_sem.at[1], at_y(1), 1).start()
            kv_send(column(-1), pc_sem.at[1], partner, 2).start()
            kv_send(column(1), yd_sem.at[0], at_y(-1), 1).wait_recv()
            kv_send(half(1, False), yd_sem.at[1], at_y(-1), 1).start()
            kv_send(column(1), pc_sem.at[2], partner, 2).start()
        elif step == 2:
            kv_send(half(2, True), yu_sem.at[1], at_y(1), 1).wait_recv()
            kv_send(half(2, False), yd_sem.at[1], at_y(-1), 1).wait_recv()
            kv_send(column(2), pc_sem.at[3], partner, 2).start()
        else:
            for k, dy in enumerate((0, -1, 1, 2)):
                other = kv.at[:, (y + dy + NY) % NY, 1 - c]
                kv_send(other, pc_sem.at[k], partner, 2).wait_recv()

    def kv_step(d):
        kv_up(d)
        if d < NZ // 2:
            kv_down(d)

    def attend(_):
        lane = lax.broadcasted_iota(jnp.int32, (SEQ, 2 * HEAD), 1)
        q = q_ref[...].astype(F32) * (HEAD**-0.5)
        q = jnp.concatenate([jnp.where(lane < HEAD, q, 0.0), jnp.where(lane < HEAD, 0.0, q)], axis=0).astype(BF)
        own_gate = gate_ref[0:1, pl.ds(pl.multiple_of(me * SEQ, SEQ), SEQ)]
        column_gate = jnp.transpose(jnp.broadcast_to(own_gate, (SEQ, SEQ)))[:, 0:1]
        gq = jnp.concatenate([column_gate, column_gate], axis=0)
        wide = NYC * SEQ

        def scored(plane):
            keys = []
            for k in range(NYC):
                block = kv[plane, k // 2, k % 2, 0:HEAD, :]
                keys.append(jnp.concatenate([block, block], axis=0))
            gk = gate_ref[0:1, pl.ds(pl.multiple_of(plane * wide, wide), wide)]
            return mm(q, jnp.concatenate(keys, axis=1)) + (gq - gk)

        def folded(w):
            total = w[:, 0:SEQ]
            for k in range(1, NYC):
                total = total + w[:, k * SEQ : (k + 1) * SEQ]
            return total

        def mixed(plane, w):
            values = []
            for k in range(NYC):
                block = kv[plane, k // 2, k % 2, HEAD : 2 * HEAD, :]
                values.append(jnp.concatenate([block, block], axis=0))
            return lax.dot_general(
                w.astype(BF), jnp.concatenate(values, axis=1), (((1,), (1,)), ((), ())), preferred_element_type=F32
            )

        rows = lax.broadcasted_iota(jnp.int32, (2 * SEQ, wide), 0) & (SEQ - 1)
        cols = lax.broadcasted_iota(jnp.int32, (2 * SEQ, wide), 1)
        s = jnp.where(cols <= rows + yc * SEQ, scored(z), -jnp.inf)
        best = jnp.max(s, axis=1, keepdims=True)
        w = jnp.exp(s - best)

        def plane_step(plane, state):
            best, total, summed = state
            s = scored(plane)
            new = jnp.maximum(best, jnp.max(s, axis=1, keepdims=True))
            factor = jnp.exp(best - new)
            w = jnp.exp(s - new)
            return new, total * factor + folded(w), summed * factor + mixed(plane, w)

        best, total, summed = lax.fori_loop(0, z, plane_step, (best, folded(w), mixed(z, w)))
        result = summed / jnp.sum(total, axis=1, keepdims=True)
        result = jnp.where(lane < HEAD, result[0:SEQ, :], result[SEQ : 2 * SEQ, :])
        att[...] = result.astype(BF)
        for k, x in enumerate((right, left, opp)):
            att_send(k, x).start()
        att_all[t] = att[pl.ds(pl.multiple_of(t * MIX, MIX), MIX), :]

    def att_send(k, x):
        return pltpu.make_async_remote_copy(
            src_ref=att.at[pl.ds(pl.multiple_of(x * MIX, MIX), MIX), :], dst_ref=att_all.at[t],
            send_sem=ts_sem, recv_sem=t_sem.at[k], device_id=(me, x), device_id_type=MESH,
        )

    def project(_):
        for k, x in enumerate((left, right, opp)):
            pltpu.make_async_remote_copy(
                src_ref=att_all.at[x], dst_ref=att_all.at[x], send_sem=ts_sem, recv_sem=t_sem.at[k],
                device_id=(me, x), device_id_type=MESH,
            ).wait_recv()
        loads[4].wait()
        joined = jnp.concatenate([att_all[k] for k in range(NT)], axis=1)
        mix_ref[...] = mm(joined, wo[...]).astype(BF)

    own = pl.ds(pl.multiple_of(t * ROWS, ROWS), ROWS)
    tokens = NT * ROWS
    r = routes_ref[...]
    r0 = r[0:1, :]
    r1 = r[1:2, :]
    expert = lax.broadcasted_iota(jnp.int32, (NE, tokens), 0)
    s0 = jnp.where(r0 == expert, 1.0, 0.0)
    s1 = jnp.where(r1 == expert, 1.0, 0.0)
    ta = lax.broadcasted_iota(jnp.int32, (tokens, tokens), 0)
    tb = lax.broadcasted_iota(jnp.int32, (tokens, tokens), 1)
    earlier = jnp.where((ta < tb) & ((ta >> 6) == (tb >> 6)), 1.0, 0.0).astype(BF)
    before = mm((s0 + s1).astype(BF), earlier)
    slot0 = r0.astype(F32) * CAP + jnp.sum(before * s0, axis=0, keepdims=True)
    slot1 = r1.astype(F32) * CAP + jnp.sum((before + s0) * s1, axis=0, keepdims=True)

    slot = lax.broadcasted_iota(jnp.int32, (SL, tokens), 0).astype(F32)
    pick[0:tokens, :] = jnp.transpose(jnp.where(slot0 == slot, 1.0, 0.0)).astype(BF)
    pick[tokens : 2 * tokens, :] = jnp.transpose(jnp.where(slot1 == slot, 1.0, 0.0)).astype(BF)
    wcol[...] = jnp.transpose(jnp.concatenate([rw_ref[...], jnp.zeros((6, tokens), F32)], axis=0))
    both = jnp.concatenate([pick[own, :], pick[pl.ds(pl.multiple_of(tokens + t * ROWS, ROWS), ROWS), :]], axis=0)

    loads[0].wait()

    def normalise(rows):
        wide = xin[rows, :].astype(F32)
        scale = lax.rsqrt(jnp.mean(wide * wide, axis=-1, keepdims=True) + 1e-06)
        normed[rows, :] = (wide * scale * gain_ref[...].astype(F32)[None, :]).astype(BF)

    normalise(own)
    chosen = jnp.transpose(both[0:ROWS, :].astype(F32) + both[ROWS : 2 * ROWS, :].astype(F32)).astype(BF)
    obuf[...] = mm(chosen, normed[own, :]).astype(BF)
    for g in range(SL // 16):
        rows_to_tiles(perm, obuf, 16 * g, send, 256 * g)

    loads[5].wait()
    loads[6].wait()
    pl.semaphore_wait(barrier, NE - 1 + 3)

    sendp4 = sendp.reshape(len(FULL) * NT, QR, 128)

    def dispatch(q):
        far = ((z + DZ[q]) % NZ) * NYC

        def ship(j, _):
            place = (yc + j) % NYC
            to = far + place
            if q in FULL:
                src = sendp4.at[
                    pl.ds(FULL.index(q) * NT, NT), pl.ds(pl.multiple_of(place * CH, CH), CH), :
                ]
                dst = recv.at[:, pl.ds(pl.multiple_of(q * QR + yc * CH, CH), CH), :]
            else:
                src = send.at[pl.ds(pl.multiple_of(to * CH, CH), CH), :]
                dst = recv.at[t, pl.ds(pl.multiple_of(q * QR + yc * CH, CH), CH), :]
            pltpu.make_async_remote_copy(
                src_ref=src, dst_ref=dst, send_sem=ap_sem if q in FULL else as_sem, recv_sem=a_sem.at[q],
                device_id=(to, t), device_id_type=MESH,
            ).start()
            return 0

        lax.fori_loop(1 if q == 0 else 0, NYC, ship, 0)

    for q in ISSUE:
        if q not in FULL:
            dispatch(q)
    recv[t, pl.ds(pl.multiple_of(yc * CH, CH), CH), :] = send[pl.ds(pl.multiple_of(me * CH, CH), CH), :]

    for b in range(NT):
        normalise(pl.ds(b * ROWS, ROWS))
    lane = lax.broadcasted_iota(jnp.int32, (BLK, tokens), 1)
    row = lax.broadcasted_iota(jnp.int32, (BLK, tokens), 0).astype(F32)
    named = []
    for q in FULL:
        goal = row + (((z + DZ[q]) % NZ) * BLK).astype(F32)
        hit = (slot0 == goal) | (slot1 == goal)
        named += [jnp.where(hit & ((lane >> 6) == b), 1.0, 0.0) for b in range(NT)]
    obuf[...] = mm(jnp.concatenate(named, axis=0).astype(BF), normed[...]).astype(BF)
    for g in range(SL // 16):
        rows_to_tiles(perm, obuf, 16 * g, sendp, 256 * g)
    for q in ISSUE:
        if q in FULL:
            dispatch(q)

    def chunk(src, q):
        return recv.at[src, pl.ds(q * QR, QR), :]

    def hop(src, q, sem, x):
        return pltpu.make_async_remote_copy(
            src_ref=chunk(src, q), dst_ref=chunk(src, q), send_sem=xs_sem, recv_sem=sem.at[q],
            device_id=(me, x), device_id_type=MESH,
        )

    def arrive(q):
        n = QR - CH if q == 0 else QR
        dst = recv.at[:, pl.ds(q * QR, n), :] if q in FULL else recv.at[t, pl.ds(q * QR, n), :]
        pltpu.make_async_remote_copy(
            src_ref=dst, dst_ref=dst,
            send_sem=as_sem, recv_sem=a_sem.at[q], device_id=(me, right), device_id_type=MESH,
        ).wait_recv()

    def spread(q):
        arrive(q)
        if q in FULL:
            return
        hop(t, q, gl_sem, right).start()
        hop(t, q, gr_sem, left).start()

    def clockwise(q):
        return PARTS.index(q) % 2 == 0

    def relay(q):
        if q in FULL:
            return
        if clockwise(q):
            hop(left, q, gl_sem, right).wait_recv()
            hop(left, q, g2_sem, right).start()
        else:
            hop(right, q, gr_sem, left).wait_recv()
            hop(right, q, g2_sem, left).start()

    def gathered(q):
        if q in FULL:
            return
        if clockwise(q):
            hop(right, q, gr_sem, left).wait_recv()
        else:
            hop(left, q, gl_sem, right).wait_recv()
        hop(opp, q, g2_sem, right).wait_recv()

    def rsend(src, dst, sem, p, x):
        return pltpu.make_async_remote_copy(
            src_ref=src, dst_ref=dst.at[p], send_sem=rr_sem, recv_sem=sem.at[p], device_id=(me, x), device_id_type=MESH
        )

    def ways(p):
        return (right, left) if p % 2 == 0 else (left, right)

    first = next(step for step in ORDER if step[0] == "experts")

    def experts(p):
        gathered(2 * p)
        gathered(2 * p + 1)
        if ("experts", p) == first:
            for load in loads[1:4]:
                load.wait()
        for tt in range(NT):
            for g in range(PT // 16):
                at = p * 2 * QR + g * 256
                y = mm(perm, recv[tt, at : at + 256, :]).astype(BF)
                row = tt * PT + 16 * g
                for i in range(TR):
                    xb[row : row + 16, 128 * i : 128 * i + 128] = y[16 * i : 16 * i + 16, :]
        x = xb[...]
        gate = mm(x, wg[...])
        up = mm(x, wu[...])
        hidden = (gate / (1.0 + jnp.exp(-gate)) * up).astype(BF)
        for tt in range(NT):
            part[p, tt] = mm(hidden[tt * PT : (tt + 1) * PT, :], wd[...]).astype(BF)
        fwd, bwd = ways(p)
        rsend(part.at[p, opp], rs1, r1_sem, p, fwd).start()
        rsend(part.at[p, bwd], rss, rss_sem, p, bwd).start()

    def middle(p):
        fwd, bwd = ways(p)
        rsend(part.at[p, opp], rs1, r1_sem, p, fwd).wait_recv()
        sumb[p] = (rs1[p].astype(F32) + part[p, fwd].astype(F32)).astype(BF)
        rsend(sumb.at[p], rsd, rsd_sem, p, fwd).start()

    def finish(p):
        fwd, bwd = ways(p)
        rsend(part.at[p, bwd], rss, rss_sem, p, bwd).wait_recv()
        rsend(sumb.at[p], rsd, rsd_sem, p, fwd).wait_recv()
        tot[...] = (part[p, t].astype(F32) + rss[p].astype(F32) + rsd[p].astype(F32)).astype(BF)
        done = 0
        for q in (2 * p, 2 * p + 1):
            while done < (q + 1 - 2 * p) * QR:
                rows_to_tiles(perm, tot, done // TR, ret, p * 2 * QR + done)
                done += 256
            far = ((z + NZ - DZ[q]) % NZ) * NYC

            def home(j, _, q=q, far=far):
                to = (yc + j) % NYC
                pltpu.make_async_remote_copy(
                    src_ref=ret.at[pl.ds(pl.multiple_of(q * QR + to * CH, CH), CH), :],
                    dst_ref=back.at[pl.ds(pl.multiple_of(me * CH, CH), CH), :],
                    send_sem=bs_sem,
                    recv_sem=b_sem,
                    device_id=(far + to, t),
                    device_id_type=MESH,
                ).start()
                return 0

            lax.fori_loop(1 if q == 0 else 0, NYC, home, 0)
        if p == 0:
            back[pl.ds(pl.multiple_of(me * CH, CH), CH), :] = ret[pl.ds(pl.multiple_of(yc * CH, CH), CH), :]

    steps = dict(
        spread=spread, relay=relay, experts=experts, middle=middle, finish=finish, kv=kv_step, rows=kv_rows,
        attend=attend, project=project,
    )
    for name, index in ORDER:
        steps[name](index)

    n = ALL - CH
    last = pltpu.make_async_remote_copy(
        src_ref=ret.at[pl.ds(0, n), :], dst_ref=back.at[pl.ds(0, n), :], send_sem=bs_sem, recv_sem=b_sem,
        device_id=(me, right), device_id_type=MESH,
    )
    last.wait_recv()
    for g in range(SL // 16):
        y = mm(perm, back[256 * g : 256 * g + 256, :]).astype(BF)
        for i in range(TR):
            resb[16 * g : 16 * g + 16, 128 * i : 128 * i + 128] = y[16 * i : 16 * i + 16, :]
    picked = mm(both, resb[...])
    w = wcol[own, :]
    out_ref[...] = (w[:, 0:1] * picked[0:ROWS, :] + w[:, 1:2] * picked[ROWS : 2 * ROWS, :]).astype(BF)

    last.wait_send()
    pltpu.make_async_remote_copy(
        src_ref=kv.at[:, pl.ds(0, 3), 0], dst_ref=kv.at[:, pl.ds(0, 3), 0], send_sem=ks_sem.at[1], recv_sem=ku_sem.at[0],
        device_id=(me, right), device_id_type=MESH,
    ).wait_send()
    pltpu.make_async_remote_copy(
        src_ref=kv.at[:, :, 0], dst_ref=kv.at[:, :, 0], send_sem=ks_sem.at[2], recv_sem=ku_sem.at[0],
        device_id=(me, right), device_id_type=MESH,
    ).wait_send()
    pltpu.make_async_remote_copy(
        src_ref=kv.at[pl.ds(0, NZ - 1), 0, 0], dst_ref=kv.at[pl.ds(0, NZ - 1), 0, 0], send_sem=ks_sem.at[0],
        recv_sem=ku_sem.at[0], device_id=(me, right), device_id_type=MESH,
    ).wait_send()
    pltpu.make_async_remote_copy(
        src_ref=att.at[pl.ds(0, 3 * MIX), :], dst_ref=att.at[pl.ds(0, 3 * MIX), :], send_sem=ts_sem,
        recv_sem=t_sem.at[0], device_id=(me, right), device_id_type=MESH,
    ).wait_send()
    n = len(PARTS) * QR - CH
    pltpu.make_async_remote_copy(
        src_ref=send.at[pl.ds(0, n), :], dst_ref=send.at[pl.ds(0, n), :], send_sem=as_sem, recv_sem=a_sem.at[0],
        device_id=(me, right), device_id_type=MESH,
    ).wait_send()
    pltpu.make_async_remote_copy(
        src_ref=sendp, dst_ref=sendp, send_sem=ap_sem, recv_sem=a_sem.at[0],
        device_id=(me, right), device_id_type=MESH,
    ).wait_send()
    n = len(PARTS) * QR
    pltpu.make_async_remote_copy(
        src_ref=recv.at[pl.ds(0, 3), pl.ds(0, n), :], dst_ref=recv.at[pl.ds(0, 3), pl.ds(0, n), :], send_sem=xs_sem,
        recv_sem=gl_sem.at[0], device_id=(me, right), device_id_type=MESH,
    ).wait_send()
    pltpu.make_async_remote_copy(
        src_ref=part.at[:, pl.ds(0, 3)], dst_ref=part.at[:, pl.ds(0, 3)], send_sem=rr_sem, recv_sem=r1_sem.at[0],
        device_id=(me, right), device_id_type=MESH,
    ).wait_send()


def hand_over(out_ref, mix_ref, out, mix, sems):
    copies = (pltpu.make_async_copy(out_ref, out, sems.at[0]), pltpu.make_async_copy(mix_ref, mix, sems.at[1]))
    for copy in copies:
        copy.start()
    for copy in copies:
        copy.wait()


def body(
    queries,
    key_cache,
    value_cache,
    cum_gate,
    out_weight,
    routed_input,
    norm_gain,
    routes,
    route_weight,
    expert_gate,
    expert_up,
    expert_down,
):
    vmem = pl.BlockSpec(memory_space=pltpu.VMEM)
    hbm = pl.BlockSpec(memory_space=pl.ANY)
    dma = pltpu.SemaphoreType.DMA
    expert_out, mixed_out = pl.pallas_call(
        layer_kernel,
        out_shape=(jax.ShapeDtypeStruct((ROWS, D), BF), jax.ShapeDtypeStruct((MIX, D), BF)),
        in_specs=[hbm, vmem, vmem, vmem, hbm, hbm, hbm, vmem, hbm, hbm, vmem, hbm],
        out_specs=(vmem, vmem),
        scratch_shapes=[
            pltpu.VMEM((NT * ROWS, D), BF),
            pltpu.VMEM((NT * ROWS, D), BF),
            pltpu.VMEM((SL, D), BF),
            pltpu.VMEM((2 * NT * ROWS, SL), BF),
            pltpu.VMEM((NT * ROWS, 8), F32),
            pltpu.VMEM((ALL, 128), BF),
            pltpu.VMEM((len(FULL) * NT * QR, 128), BF),
            pltpu.VMEM((NT, ALL, 128), BF),
            pltpu.VMEM((D, HID), BF),
            pltpu.VMEM((D, HID), BF),
            pltpu.VMEM((HID, D), BF),
            pltpu.VMEM((NT * PT, D), BF),
            pltpu.VMEM((NP, NT, PT, D), BF),
            pltpu.VMEM((NP, PT, D), BF),
            pltpu.VMEM((NP, PT, D), BF),
            pltpu.VMEM((NP, PT, D), BF),
            pltpu.VMEM((NP, PT, D), BF),
            pltpu.VMEM((PT, D), BF),
            pltpu.VMEM((ALL, 128), BF),
            pltpu.VMEM((ALL, 128), BF),
            pltpu.VMEM((SL, D), BF),
            pltpu.VMEM((NZ, NY, 2, 2 * HEAD, SEQ), BF),
            pltpu.VMEM((NT * 2 * HEAD, D), BF),
            pltpu.VMEM((SEQ, 2 * HEAD), BF),
            pltpu.VMEM((NT, MIX, 2 * HEAD), BF),
            dma((7,)),
            dma,
            dma,
            dma((NZ,)),
            dma,
            dma((NZ,)),
            dma((NZ,)),
            dma((NZ,)),
            dma,
            dma((NP,)),
            dma((NP,)),
            dma((NP,)),
            dma,
            dma,
            dma((3,)),
            dma((4,)),
            dma((3,)),
            dma((2,)),
            dma((2,)),
            dma((4,)),
            dma,
            dma((3,)),
        ],
        compiler_params=pltpu.CompilerParams(collective_id=0, has_side_effects=True, vmem_limit_bytes=67043328),
        cost_estimate=pl.CostEstimate(flops=60_000_000_000, bytes_accessed=8_000_000, transcendentals=0),
        name="layer",
    )(
        routed_input, routes.T, route_weight.T, norm_gain,
        expert_gate[0], expert_up[0], expert_down[0],
        queries, key_cache[0], value_cache[0], cum_gate, out_weight,
    )
    expert_out, mixed_out = pl.pallas_call(
        hand_over,
        out_shape=(jax.ShapeDtypeStruct((ROWS, D), BF), jax.ShapeDtypeStruct((MIX, D), BF)),
        in_specs=[vmem] * 2,
        out_specs=(hbm, hbm),
        scratch_shapes=[dma((2,))],
        compiler_params=pltpu.CompilerParams(vmem_limit_bytes=67043328),
        name="hand_over",
    )(expert_out, mixed_out)
    return (mixed_out, expert_out)


def solution(mesh):
    return jax.shard_map(
        body,
        mesh=mesh,
        in_specs=(
            P("ep", "tp"),
            P("tp", None, "ep"),
            P("tp", None, "ep"),
            P("tp", None),
            P(),
            P("ep", None),
            P(),
            P("ep", None),
            P("ep", None),
            P("ep", None, "tp"),
            P("ep", None, "tp"),
            P("ep", "tp", None),
        ),
        out_specs=(P(("ep", "tp"), None), P(("ep", "tp"), None)),
        check_vma=False,
    )
```
